256 devices in a mesh: grp: 2 (over y), ep: 32 (over z, core), tp: 4 (over x).
Axes of the slice: x: 4, y: 2, z: 16, core: 2. Of those that a mesh axis runs over, the one named last changes fastest.
The devices are a block of a 4x16x16 slice.
Arguments:
- queries: bfloat16 [32768, 1024], P(('grp', 'ep'), 'tp'), parts along dimension 0, may hold values from -6 to 6
- key_rows: bfloat16 [32768, 512], P(('grp', 'ep'), 'tp'), parts along dimension 0, may hold values from -6 to 6
- value_rows: bfloat16 [32768, 512], P(('grp', 'ep'), 'tp'), parts along dimension 0, may hold values from -6 to 6
- query_gain: float32 [128], replicated, may hold values from 0.3 to 9
- key_gain: float32 [128], replicated, may hold values from 0.3 to 9
- log_forget: float32 [8, 32768], P('tp', 'grp'), parts along dimension 1, may hold values from -16384 to 0, as said below
- out_weight: bfloat16 [1024, 2048], P('tp'), may hold values from -0.1875 to 0.1875
- expert_rows: bfloat16 [32768, 2048], P(('grp', 'ep')), parts along dimension 0, may hold values from -6 to 6
- expert_gain: float32 [2048], replicated, may hold values from 0.1 to 1.9
- routes: int32 [2, 32768], P(None, ('grp', 'ep')), parts along dimension 1, may hold values from 0 to 31, as said below
- route_weight: float32 [2, 32768], P(None, ('grp', 'ep')), parts along dimension 1, may hold values from 0.1 to 1
- gate_weight: bfloat16 [32, 2048, 1024], P('ep', None, 'tp'), may hold values from -0.125 to 0.125
- up_weight: bfloat16 [32, 2048, 1024], P('ep', None, 'tp'), may hold values from -0.125 to 0.125
- down_weight: bfloat16 [32, 1024, 2048], P('ep', 'tp'), may hold values from -0.1875 to 0.1875
Outputs:
- mixer_out: bfloat16 [32768, 2048], P(('grp', 'ep', 'tp')), parts along dimension 0
- expert_out: bfloat16 [32768, 2048], P(('grp', 'ep'), 'tp'), parts along dimension 0
The draws below stay inside these ranges and needn't reach their ends.
There are 2 independent parts, one for each index of `grp`. The reference program is written for one: setup_inputs(seed, part) draws one part's arguments, and reference() takes and returns one part's arrays. A program takes and returns all parts, laid end to end along the dimension named above; an argument that names none is the same for every part. Nothing has to cross between parts.
Inputs may be any that keep to these rules, and one draw needn't show every extreme that they name: `log_forget`: each head's values never rise along the positions. `routes`: the 2 experts of a token differ and lie in one group of 8 consecutive numbers. Among the tokens of one index of ep (512 consecutive tokens), no expert is named more than 48 times, and in every draw some experts are named exactly 48 times in every such block.
All inputs are finite; a program needn't handle non-finite values.
Results may differ from the reference program's by a relative error of at most 0.012.
The reference program's roundings to bfloat16 on the way count: a program that leaves them out, or rounds other values in their place, can miss the bound.
Values may be sent and summed in bfloat16 or wider, within the bound.
No kernel may reach another device: no remote copies, remote signals or barrier semaphores. Data moves between devices by JAX's collectives and lax.ppermute only.
A program may use at most 128 MiB of HBM per device.

```python
import math
import jax
import jax.numpy as jnp
from jax import lax

D = 2048
QUERY_HEADS = 8
KV_HEADS = 4
HEAD_SIZE = 128
EXPERTS = 32
GROUP_SIZE = 8
FF = 1024
TOP = 2
SPAN = 512
SEQUENCE_TOKENS = 16384
CAP = 48
N_EP = 32
N_TP = 4


def gain_draw(gain_key):
    return jnp.clip(1.0 + 0.18 * jax.random.normal(gain_key, (HEAD_SIZE,), jnp.float32), 0.3, 1.7)


def draw_query_gain(key, part):
    return gain_draw(jax.random.fold_in(key, 3))


def draw_key_gain(key, part):
    return gain_draw(jax.random.fold_in(key, 5))


def draw_log_forget(key, part):
    divided_keys = jax.random.split(jax.random.fold_in(key, 7), 7)
    token_position = jnp.arange(SEQUENCE_TOKENS, dtype=jnp.int32)
    shard_factor = jnp.exp(jax.random.uniform(divided_keys[0], (SEQUENCE_TOKENS // SPAN,), jnp.float32, -0.7, 0.7))
    factor_vector = jnp.repeat(shard_factor, SPAN)
    fast_rank = jax.random.permutation(divided_keys[1], QUERY_HEADS).astype(jnp.int32)
    is_fast = fast_rank < QUERY_HEADS // 2
    slow_rate = jax.random.uniform(divided_keys[2], (QUERY_HEADS,), jnp.float32, 0.3, 0.9) / SEQUENCE_TOKENS
    fast_rate = 1.0 / jax.random.uniform(divided_keys[3], (QUERY_HEADS,), jnp.float32, 30.0, 50.0)
    baseline_rate = jnp.where(is_fast, fast_rate, slow_rate)
    jitter_amount = jax.random.uniform(divided_keys[4], (QUERY_HEADS, SEQUENCE_TOKENS), jnp.float32, 0.5, 1.5)
    spike_position = jax.random.randint(divided_keys[5], (QUERY_HEADS, 3), 0, SEQUENCE_TOKENS)
    spike_length = -jnp.log(jax.random.uniform(divided_keys[6], (QUERY_HEADS, 3), jnp.float32, 0.6, 0.8))
    spike_events = jnp.sum(jnp.where(token_position[None, None, :] == spike_position[:, :, None], spike_length[:, :, None], 0.0), axis=1)
    logarithm_step = -(baseline_rate[:, None] * factor_vector[None, :] * jitter_amount + spike_events)
    return jnp.cumsum(logarithm_step, axis=1)


def route_block(block_key, full_group):
    divided_keys = jax.random.split(block_key, 4)
    full_rows = GROUP_SIZE * CAP // 2
    rest_rows = SPAN - full_rows
    other_sizes = jnp.array([rest_rows // 2, rest_rows // 3, rest_rows - rest_rows // 2 - rest_rows // 3], jnp.int32)
    others = (full_group + 1 + jax.random.permutation(divided_keys[0], 3).astype(jnp.int32)) % 4
    group_sizes = jnp.zeros((4,), jnp.int32).at[full_group].set(full_rows).at[others].set(other_sizes)
    group_ends = jnp.cumsum(group_sizes)
    token_position = jnp.arange(SPAN, dtype=jnp.int32)
    group_of = jnp.sum((token_position[:, None] >= group_ends[None, :]).astype(jnp.int32), axis=1)
    within = token_position - (group_ends - group_sizes)[group_of]
    orders = jax.vmap(lambda sub_key: jax.random.permutation(sub_key, GROUP_SIZE).astype(jnp.int32))(jax.random.split(divided_keys[1], 4))
    shifts = jax.random.randint(divided_keys[2], (4,), 0, GROUP_SIZE - 1)
    first_pick = orders[group_of, within % GROUP_SIZE]
    second_pick = orders[group_of, (within + 1 + (within // GROUP_SIZE + shifts[group_of]) % (GROUP_SIZE - 1)) % GROUP_SIZE]
    chosen = jnp.stack([group_of * GROUP_SIZE + first_pick, group_of * GROUP_SIZE + second_pick])
    shuffle = jax.random.permutation(divided_keys[3], SPAN)
    return chosen[:, shuffle]


def draw_routes(key, part):
    full_group = jax.random.randint(jax.random.fold_in(key, 11), (), 0, 4)
    block_keys = jax.random.split(jax.random.fold_in(key, 12), SEQUENCE_TOKENS // SPAN)
    blocks = jax.vmap(lambda block_key: route_block(block_key, full_group))(block_keys)
    return jnp.transpose(blocks, (1, 0, 2)).reshape(2, SEQUENCE_TOKENS).astype(jnp.int32)


def steps_of(key, dims, cuts, smallest, high):
    def one(position, parts):
        draws = jax.random.uniform(jax.random.fold_in(jax.random.fold_in(key, 6), position), (parts,), jnp.float32, smallest / len(cuts), high / len(cuts))
        return jnp.repeat(jnp.exp(draws), dims[position] // parts).reshape((-1,) + (1,) * (len(dims) - position - 1))

    factor_of = one(*cuts[0])
    for cut in cuts[1:]:
        factor_of = factor_of * one(*cut)
    return factor_of


def noise(rng, shape, spread, bound, cuts=(), held_as=jnp.bfloat16):
    result = jax.random.normal(rng, shape, jnp.float32) * spread
    if len(cuts) > 0:
        result = steps_of(rng, shape, cuts, -0.22, 0.18) * result
    return jnp.clip(result, min=-bound, max=bound).astype(held_as)


def setup_inputs(seed: int = 0, part: int = 0) -> dict:
    keys = jax.random.split(jax.random.key(seed), 15)
    part_keys = jax.random.split(jax.random.fold_in(keys[14], part), 15)
    return {
        "queries": noise(part_keys[0], (SEQUENCE_TOKENS, QUERY_HEADS * HEAD_SIZE), 1.0, 6.0, ((0, 32), (1, 4))),
        "key_rows": noise(part_keys[1], (SEQUENCE_TOKENS, KV_HEADS * HEAD_SIZE), 1.0, 6.0, ((0, 32), (1, 4))),
        "value_rows": noise(part_keys[2], (SEQUENCE_TOKENS, KV_HEADS * HEAD_SIZE), 1.0, 6.0, ((0, 32), (1, 4))),
        "query_gain": draw_query_gain(jax.random.fold_in(keys[14], 71), part),
        "key_gain": draw_key_gain(jax.random.fold_in(keys[14], 71), part),
        "log_forget": draw_log_forget(jax.random.fold_in(jax.random.fold_in(keys[14], part), 71), part),
        "out_weight": noise(keys[6], (QUERY_HEADS * HEAD_SIZE, D), (QUERY_HEADS * HEAD_SIZE) ** -0.5, 0.1875, ((0, 4),)),
        "expert_rows": noise(part_keys[7], (SEQUENCE_TOKENS, D), 1.0, 6.0, ((0, 32),)),
        "expert_gain": jnp.clip(1.0 + 0.18 * jax.random.normal(keys[8], (D,), jnp.float32), 0.1, 1.9),
        "routes": draw_routes(jax.random.fold_in(jax.random.fold_in(keys[14], part), 71), part),
        "route_weight": jnp.clip(jnp.exp(math.log(1.0) - 2.3025851 * jax.random.uniform(part_keys[10], (TOP, SEQUENCE_TOKENS), jnp.float32) ** steps_of(part_keys[10], (TOP, SEQUENCE_TOKENS), ((1, 32),), -0.2, 0.2)), 0.1, 1.0),
        "gate_weight": noise(keys[11], (EXPERTS, D, FF), D ** -0.5, 0.125, ((0, 32), (2, 4))),
        "up_weight": noise(keys[12], (EXPERTS, D, FF), D ** -0.5, 0.125, ((0, 32), (2, 4))),
        "down_weight": noise(keys[13], (EXPERTS, FF, D), FF ** -0.5, 0.1875, ((0, 32), (1, 4))),
    }


def head_norm(inputs, scale_gain):
    widened = inputs.astype(jnp.float32)
    factor = lax.rsqrt(lax.optimization_barrier(jnp.mean(widened * widened, axis=-1, keepdims=True)) + 1e-06)
    return widened * factor * scale_gain.astype(jnp.float32)

def slot_table(chosen, experts_all, capacity):
    n_rows = chosen.shape[0]
    per_row = chosen.shape[1]
    flat_ids = chosen.reshape(-1)
    one_hot = (flat_ids[:, None] == jnp.arange(experts_all, dtype=jnp.int32)[None, :]).astype(jnp.int32)
    within = lax.optimization_barrier(jnp.sum((jnp.cumsum(one_hot, axis=0) - 1) * one_hot, axis=1))
    slot_index = (flat_ids * capacity + within).astype(jnp.int32)
    row_of = jnp.arange(n_rows * per_row, dtype=jnp.int32) // per_row
    slot_owner = jnp.full((experts_all * capacity,), n_rows, jnp.int32).at[slot_index].set(row_of)
    return (slot_index.reshape(n_rows, per_row), slot_owner)

def reference(queries, key_rows, value_rows, query_gain, key_gain, log_forget, out_weight, expert_rows, expert_gain, routes, route_weight, gate_weight, up_weight, down_weight):
    span_len = SEQUENCE_TOKENS // N_EP
    group_ratio = QUERY_HEADS // KV_HEADS
    scale_qk = HEAD_SIZE ** (-0.5)
    q_all = lax.optimization_barrier(head_norm(queries.reshape(SEQUENCE_TOKENS, KV_HEADS, group_ratio, HEAD_SIZE), query_gain).astype(jnp.bfloat16)).astype(jnp.float32)
    k_all = lax.optimization_barrier(head_norm(key_rows.reshape(SEQUENCE_TOKENS, KV_HEADS, HEAD_SIZE), key_gain).astype(jnp.bfloat16)).astype(jnp.float32)
    v_all = value_rows.reshape(SEQUENCE_TOKENS, KV_HEADS, HEAD_SIZE).astype(jnp.float32)
    positions = jnp.arange(span_len, dtype=jnp.int32)

    def query_block(block_index):
        q_here = lax.dynamic_slice_in_dim(q_all, block_index * span_len, span_len, 0)
        gates_here = lax.dynamic_slice_in_dim(log_forget, block_index * span_len, span_len, 1)
        gates_here = gates_here.T.reshape(span_len, KV_HEADS, group_ratio)

        def key_step(key_index, running):
            run_max, run_sum, run_acc = running
            k_here = lax.dynamic_slice_in_dim(k_all, key_index * span_len, span_len, 0)
            v_here = lax.dynamic_slice_in_dim(v_all, key_index * span_len, span_len, 0)
            key_gates = lax.dynamic_slice_in_dim(log_forget, key_index * span_len, span_len, 1)
            key_gates = key_gates.reshape(KV_HEADS, group_ratio, span_len)
            scores = jnp.einsum('qgrd,kgd->qgrk', q_here, k_here) * scale_qk
            scores = scores + gates_here[..., None] - key_gates[None]
            visible = (key_index * span_len + positions)[None, :] <= (block_index * span_len + positions)[:, None]
            scores = jnp.where(visible[:, None, None, :], scores, -jnp.inf)
            new_max = jnp.maximum(run_max, lax.optimization_barrier(jnp.max(scores, axis=-1)))
            shrink = jnp.exp(run_max - new_max)
            weights = jnp.exp(scores - new_max[..., None])
            run_sum = shrink * run_sum + lax.optimization_barrier(jnp.sum(weights, axis=-1))
            weights_low = lax.optimization_barrier(weights.astype(jnp.bfloat16)).astype(jnp.float32)
            gathered = jnp.einsum('qgrk,kgd->qgrd', weights_low, v_here)
            return (new_max, run_sum, shrink[..., None] * run_acc + gathered)
        start_state = (jnp.full((span_len, KV_HEADS, group_ratio), -jnp.inf, jnp.float32), jnp.zeros((span_len, KV_HEADS, group_ratio), jnp.float32), jnp.zeros((span_len, KV_HEADS, group_ratio, HEAD_SIZE), jnp.float32))
        run_max, run_sum, run_acc = lax.fori_loop(0, block_index + 1, key_step, start_state)
        return (run_acc / run_sum[..., None]).astype(jnp.bfloat16)
    attended = lax.map(query_block, jnp.arange(N_EP, dtype=jnp.int32))
    attended = attended.reshape(SEQUENCE_TOKENS, QUERY_HEADS * HEAD_SIZE)
    mixer_out = jnp.dot(attended, out_weight, preferred_element_type=jnp.float32).astype(jnp.bfloat16)
    normed = head_norm(expert_rows, expert_gain).astype(jnp.bfloat16)
    block_routes = routes.reshape(TOP, N_EP, span_len).transpose(1, 2, 0)
    slot_all, owner_all = jax.vmap(lambda chosen: slot_table(chosen, EXPERTS, CAP))(block_routes)
    block_base = jnp.arange(N_EP, dtype=jnp.int32)[:, None] * span_len
    global_rows = jnp.where(owner_all == span_len, SEQUENCE_TOKENS, owner_all + block_base).astype(jnp.int32)
    row_index = global_rows.reshape(N_EP, EXPERTS, CAP).transpose(1, 0, 2).reshape(EXPERTS, N_EP * CAP)
    padded = jnp.concatenate([normed, jnp.zeros((1, D), jnp.bfloat16)], axis=0)
    ff_part = FF // N_TP

    def one_expert(inputs):
        index_rows, w_gate, w_up, w_down = inputs
        taken = padded[index_rows]
        gate_part = jnp.dot(taken, w_gate, preferred_element_type=jnp.float32)
        up_part = jnp.dot(taken, w_up, preferred_element_type=jnp.float32)
        hidden = (jax.nn.silu(gate_part) * up_part).astype(jnp.bfloat16)
        running = jnp.zeros((N_EP * CAP, D), jnp.float32)
        for part_index in range(N_TP):
            piece = jnp.dot(hidden[:, part_index * ff_part:(part_index + 1) * ff_part], w_down[part_index * ff_part:(part_index + 1) * ff_part], preferred_element_type=jnp.float32)
            running = running + lax.optimization_barrier(piece.astype(jnp.bfloat16)).astype(jnp.float32)
        return running.astype(jnp.bfloat16)
    results = lax.map(one_expert, (row_index, gate_weight, up_weight, down_weight))
    result_table = results.reshape(EXPERTS, N_EP, CAP, D)
    expert_of = slot_all // CAP
    cell_of = slot_all % CAP
    block_id = jnp.arange(N_EP, dtype=jnp.int32)[:, None, None]
    picked = result_table[expert_of, block_id, cell_of]
    weights_all = route_weight.reshape(TOP, N_EP, span_len).transpose(1, 2, 0)
    expert_out = lax.optimization_barrier(jnp.sum(picked.astype(jnp.float32) * weights_all[..., None], axis=2))
    expert_out = expert_out.astype(jnp.bfloat16).reshape(SEQUENCE_TOKENS, D)
    return (mixer_out, expert_out)
```

```python
import functools

import jax
import jax.numpy as jnp
from jax import lax
from jax.experimental import pallas as pl
from jax.experimental.pallas import tpu as pltpu
from jax.sharding import Mesh
from jax.sharding import PartitionSpec as P

HEAD_SIZE = 128
EXPERTS = 32
TOP = 2
CORES = 2
EP = ("ep_0", "ep_1")
GRP_EP = ("grp", "ep_0", "ep_1")
GRP_EP_TP = ("grp", "ep_0", "ep_1", "tp")
LOG2E = 1.4426950408889634
MIB = 1024 * 1024


SMEM = pl.BlockSpec(memory_space=pltpu.SMEM)
VMEM = pl.BlockSpec(memory_space=pltpu.VMEM)
ANY = pl.BlockSpec(memory_space=pl.ANY)


def cost(flops, bytes_accessed, transcendentals=0):
    return pl.CostEstimate(
        flops=int(flops), bytes_accessed=int(bytes_accessed), transcendentals=int(transcendentals)
    )


def params(limit_mib):
    return pltpu.CompilerParams(vmem_limit_bytes=limit_mib * MIB)


def head_norm(inputs, scale_gain):
    widened = inputs.astype(jnp.float32)
    factor = lax.rsqrt(jnp.mean(widened * widened, axis=-1, keepdims=True) + 1e-06)
    return widened * factor * scale_gain


def dispatch_kernel(half, where_ref, rows_ref, gain_ref, routes_ref, out_ref, normed_ref):
    tp_index = where_ref[0]
    n_rows, width = rows_ref.shape
    step = 64

    def norm_step(i, carry):
        part = pl.ds(pl.multiple_of(i * step, step), step)
        normed_ref[part, :] = head_norm(rows_ref[part, :], gain_ref[...]).astype(jnp.bfloat16)
        return carry

    lax.fori_loop(0, n_rows // step, norm_step, 0)
    ids = routes_ref[...]
    expert_iota = lax.broadcasted_iota(jnp.int32, (EXPERTS, n_rows), 0)
    before = jnp.where(
        lax.broadcasted_iota(jnp.int32, (n_rows, n_rows), 0)
        < lax.broadcasted_iota(jnp.int32, (n_rows, n_rows), 1),
        1.0,
        0.0,
    ).astype(jnp.bfloat16)
    base = jnp.zeros((EXPERTS, 1), jnp.float32)
    targets = []
    for j in range(TOP):
        picked = ids[j : j + 1, :]
        one_hot = jnp.where(expert_iota == picked, 1.0, 0.0)
        rank = base + jnp.dot(
            one_hot.astype(jnp.bfloat16), before, preferred_element_type=jnp.float32
        )
        within = jnp.sum(one_hot * rank, axis=0, keepdims=True).astype(jnp.int32)
        base = base + jnp.sum(one_hot, axis=1, keepdims=True)
        low = (tp_index & 1) * half
        mine = ((picked & 1) == (tp_index >> 1)) & (within >= low) & (within < low + half)
        targets.append(jnp.where(mine, (picked >> 1) * half + within - low, -1))
    out_rows = out_ref.shape[0]
    row_iota = lax.broadcasted_iota(jnp.int32, (out_rows, n_rows), 0)
    select = jnp.where((row_iota == targets[0]) | (row_iota == targets[1]), 1.0, 0.0).astype(
        jnp.bfloat16
    )
    span = 512
    for start in range(0, width, span):
        cols = slice(start, start + span)
        out_ref[:, cols] = jnp.dot(
            select, normed_ref[:, cols], preferred_element_type=jnp.float32
        ).astype(jnp.bfloat16)


def dispatch_rows(where, expert_rows, gain, routes, half):
    n_rows, width = expert_rows.shape
    out_rows = EXPERTS // CORES * half
    return pl.pallas_call(
        functools.partial(dispatch_kernel, half),
        out_shape=jax.ShapeDtypeStruct((out_rows, width), jnp.bfloat16),
        in_specs=[SMEM, VMEM, VMEM, VMEM],
        out_specs=VMEM,
        scratch_shapes=[pltpu.VMEM((n_rows, width), jnp.bfloat16)],
        compiler_params=params(24),
        cost_estimate=cost(2 * out_rows * n_rows * width, 2 * (n_rows + out_rows) * width),
        name="dispatch",
    )(where, expert_rows, gain, routes)


def combine_kernel(capacity, first_ref, second_ref, routes_ref, weight_ref, out_ref):
    n_rows = out_ref.shape[0]
    ids = routes_ref[...]
    expert_iota = lax.broadcasted_iota(jnp.int32, (n_rows, EXPERTS), 1)
    before = jnp.where(
        lax.broadcasted_iota(jnp.int32, (n_rows, n_rows), 1)
        < lax.broadcasted_iota(jnp.int32, (n_rows, n_rows), 0),
        1.0,
        0.0,
    ).astype(jnp.bfloat16)
    base = jnp.zeros((1, EXPERTS), jnp.float32)
    slots = []
    for j in range(TOP):
        picked = ids[:, j : j + 1]
        one_hot = jnp.where(expert_iota == picked, 1.0, 0.0)
        rank = base + jnp.dot(
            before, one_hot.astype(jnp.bfloat16), preferred_element_type=jnp.float32
        )
        within = jnp.sum(one_hot * rank, axis=1, keepdims=True).astype(jnp.int32)
        base = base + jnp.sum(one_hot, axis=0, keepdims=True)
        slots.append(picked * capacity + within)
    slot_iota = lax.broadcasted_iota(jnp.int32, (n_rows, EXPERTS * capacity), 1)
    selects = [jnp.where(slot_iota == s, 1.0, 0.0).astype(jnp.bfloat16) for s in slots]
    width = first_ref.shape[1]
    for u, table in enumerate((first_ref, second_ref)):
        total = jnp.zeros((n_rows, width), jnp.float32)
        for j in range(TOP):
            rows = jnp.dot(selects[j], table[...], preferred_element_type=jnp.float32)
            total = total + weight_ref[:, j : j + 1] * rows
        out_ref[:, u * width : (u + 1) * width] = total.astype(jnp.bfloat16)


def combine_rows(first, second, routes_t, weight_t, capacity):
    n_rows = routes_t.shape[0]
    slots, width = first.shape
    return pl.pallas_call(
        functools.partial(combine_kernel, capacity),
        out_shape=jax.ShapeDtypeStruct((n_rows, 2 * width), jnp.bfloat16),
        in_specs=[VMEM] * 4,
        out_specs=VMEM,
        compiler_params=params(32),
        cost_estimate=cost(8 * n_rows * slots * width, 4 * slots * width),
        name="combine",
    )(first, second, routes_t, weight_t)


def expert_kernel(where_ref, x_ref, *refs):
    sources = [refs[3 * i : 3 * i + 3] for i in range(6)]
    outs = refs[18:20]
    gate_buf, up_buf, down_buf, hidden_ref, acc_ref, sems = refs[20:]
    bufs = (gate_buf, up_buf, down_buf)
    core, tp_index = where_ref[1], where_ref[0]
    home = core == (tp_index >> 1)

    def fetch(place, source):
        for i in range(3):
            pltpu.make_async_copy(source[i], bufs[i].at[place], sems.at[place, i]).start()

    pl.when(home)(lambda: fetch(0, sources[0]))
    pl.when(jnp.logical_not(home))(lambda: fetch(0, sources[1]))
    fetch(1, sources[2])
    fetch(2, sources[3])
    pl.when(core == 1)(lambda: fetch(3, sources[4]))
    pl.when(core == 0)(lambda: fetch(3, sources[5]))

    n_rows = x_ref.shape[0]
    depth = acc_ref.shape[1]
    half_rows = n_rows // 2
    acc_ref[...] = jnp.zeros_like(acc_ref)

    def shard(p, carry):
        for i in range(3):
            pltpu.make_async_copy(sources[2][i], bufs[i].at[p], sems.at[p, i]).wait()
        for part in range(2):
            rows = slice(part * half_rows, (part + 1) * half_rows)
            x = x_ref[rows, :]
            gate = jnp.dot(x, gate_buf[p], preferred_element_type=jnp.float32)
            up = jnp.dot(x, up_buf[p], preferred_element_type=jnp.float32)
            hidden_ref[rows, :] = (gate / (1.0 + jnp.exp(-gate)) * up).astype(jnp.bfloat16)
        for start in range(0, depth, 512):
            cols = slice(start, start + 512)
            piece = jnp.dot(
                hidden_ref[...], down_buf[p, :, cols], preferred_element_type=jnp.float32
            )
            acc_ref[:, cols] += piece.astype(jnp.bfloat16).astype(jnp.float32)
        return carry

    lax.fori_loop(0, gate_buf.shape[0], shard, 0)
    chips, n_tp, block, width = outs[0].shape

    def put(chip, carry):
        rows = pl.ds(pl.multiple_of(chip * block, 8), block)
        for u in range(2):
            for t in range(n_tp):
                start = (t * 2 + u) * width
                outs[u][chip, t] = acc_ref[rows, start : start + width].astype(jnp.bfloat16)
        return carry

    lax.fori_loop(0, chips, put, 0)


def expert_rows_out(where, x, shards, chips, n_tp):
    n_rows, depth = x.shape
    ff_part = shards[0].shape[1]
    width = depth // n_tp // 2
    out = jax.ShapeDtypeStruct((chips, n_tp, n_rows // chips, width), jnp.bfloat16)
    return pl.pallas_call(
        expert_kernel,
        out_shape=(out, out),
        in_specs=[SMEM, VMEM] + [ANY] * len(shards),
        out_specs=(VMEM, VMEM),
        scratch_shapes=[
            pltpu.VMEM((n_tp, depth, ff_part), jnp.bfloat16),
            pltpu.VMEM((n_tp, depth, ff_part), jnp.bfloat16),
            pltpu.VMEM((n_tp, ff_part, depth), jnp.bfloat16),
            pltpu.VMEM((n_rows, ff_part), jnp.bfloat16),
            pltpu.VMEM((n_rows, depth), jnp.float32),
            pltpu.SemaphoreType.DMA((n_tp, 3)),
        ],
        compiler_params=params(40),
        cost_estimate=cost(
            6 * n_rows * depth * ff_part * n_tp, 6 * n_tp * depth * ff_part + 4 * n_rows * depth
        ),
        name="experts",
    )(where, x, *shards)


def attention_kernel(
    where_ref, q_ref, gain_ref, own_ref, other_ref, gates_ref, out_ref, q_buf, max_ref, sum_ref, acc_ref
):
    chip, core = where_ref[2], where_ref[1]
    span = q_ref.shape[0]
    heads = q_ref.shape[1] // HEAD_SIZE
    scale = HEAD_SIZE ** (-0.5) * LOG2E
    my_block = chip * CORES + core

    def gate_row(r, block):
        return gates_ref[r : r + 1, pl.ds(pl.multiple_of(block * span, span), span)]

    origin = []
    for r in range(heads):
        cols = slice(r * HEAD_SIZE, (r + 1) * HEAD_SIZE)
        q_buf[r] = head_norm(q_ref[:, cols], gain_ref[...]).astype(jnp.bfloat16)
        origin.append(gate_row(r, my_block)[:, 0:1])

    def scores(r, kv_ref, place, block):
        product = lax.dot_general(
            q_buf[r],
            kv_ref[place, :, 0:HEAD_SIZE],
            (((1,), (1,)), ((), ())),
            preferred_element_type=jnp.float32,
        )
        return product * scale + (origin[r] - gate_row(r, block)) * LOG2E

    def weighted(prob, kv_ref, place):
        return jnp.dot(
            prob.astype(jnp.bfloat16),
            kv_ref[place, :, HEAD_SIZE : 2 * HEAD_SIZE],
            preferred_element_type=jnp.float32,
        )

    def first(r):
        logits = scores(r, own_ref, chip, my_block)
        row = lax.broadcasted_iota(jnp.int32, (span, span), 0)
        col = lax.broadcasted_iota(jnp.int32, (span, span), 1)
        logits = jnp.where(col <= row, logits, -jnp.inf)
        top = jnp.max(logits, axis=1, keepdims=True)
        prob = jnp.exp2(logits - top)
        max_ref[r] = top
        sum_ref[r] = jnp.sum(prob, axis=1, keepdims=True)
        acc_ref[r] = weighted(prob, own_ref, chip)

    def update(r, parts):
        logits = [scores(r, ref, place, block) for ref, place, block in parts]
        old = max_ref[r]
        top = old
        for part in logits:
            top = jnp.maximum(top, jnp.max(part, axis=1, keepdims=True))
        shrink = jnp.exp2(old - top)
        total = shrink * sum_ref[r]
        acc = shrink * acc_ref[r]
        for part, (ref, place, block) in zip(logits, parts):
            prob = jnp.exp2(part - top)
            total = total + jnp.sum(prob, axis=1, keepdims=True)
            acc = acc + weighted(prob, ref, place)
        max_ref[r] = top
        sum_ref[r] = total
        acc_ref[r] = acc

    for r in range(heads):
        first(r)

    @pl.when(core == 1)
    def _():
        for r in range(heads):
            update(r, [(other_ref, chip, my_block - 1)])

    def step(place, carry):
        for r in range(heads):
            update(
                r,
                [
                    (own_ref, place, place * CORES + core),
                    (other_ref, place, place * CORES + 1 - core),
                ],
            )
        return carry

    lax.fori_loop(0, chip, step, 0)
    for r in range(heads):
        cols = slice(r * HEAD_SIZE, (r + 1) * HEAD_SIZE)
        out_ref[:, cols] = (acc_ref[r] / sum_ref[r]).astype(jnp.bfloat16)


def attention(where, queries, query_gain, kv_own, kv_other, gates):
    span, width = queries.shape
    heads = width // HEAD_SIZE
    keys = gates.shape[1]
    return pl.pallas_call(
        attention_kernel,
        out_shape=jax.ShapeDtypeStruct((span, width), jnp.bfloat16),
        in_specs=[SMEM] + [VMEM] * 5,
        out_specs=VMEM,
        scratch_shapes=[
            pltpu.VMEM((heads, span, HEAD_SIZE), jnp.bfloat16),
            pltpu.VMEM((heads, span, 1), jnp.float32),
            pltpu.VMEM((heads, span, 1), jnp.float32),
            pltpu.VMEM((heads, span, HEAD_SIZE), jnp.float32),
        ],
        compiler_params=params(40),
        cost_estimate=cost(8 * span * keys * width, 4 * keys * HEAD_SIZE, span * keys * heads),
        name="attention",
    )(where, queries, query_gain, kv_own, kv_other, gates)


def shard_moves(n_tp):
    at = lambda core, t: core * n_tp + t
    near, over, up = [], [], []
    for core in range(CORES):
        for t in range(n_tp):
            if t // 2 == core:
                near.append((at(core, t), at(0, t ^ 1)))
                over.append((at(core, t), at(1 - core, t)))
            else:
                near.append((at(core, t), at(1, n_tp - 1 - t)))
    swap = [(at(c, t), at(1 - c, t)) for c in range(CORES) for t in range(n_tp)]
    pair = [(at(1, t), at(1, t ^ 1)) for t in range(n_tp)]
    down = [(at(1, t), at(0, t)) for t in range(n_tp)]
    return near, over, swap, pair, down


def on_device(
    queries,
    key_rows,
    value_rows,
    query_gain,
    key_gain,
    log_forget,
    out_weight,
    expert_rows,
    expert_gain,
    routes,
    route_weight,
    gate_weight,
    up_weight,
    down_weight,
):
    n_tp = lax.axis_size("tp")
    chips = lax.axis_size("ep_0")
    chip, core, tp_index = (lax.axis_index(a) for a in ("ep_0", "ep_1", "tp"))
    where = jnp.stack([tp_index, core, chip]).astype(jnp.int32)
    span_rows, model_width = expert_rows.shape
    capacity = n_tp * ((3 * (span_rows // n_tp) * TOP + 2 * EXPERTS - 1) // (2 * EXPERTS))
    half = capacity // 2
    row = ("ep_1", "tp")

    near, over, swap, pair, down = shard_moves(n_tp)
    mine = (gate_weight[0], up_weight[0], down_weight[0])
    near_w = [lax.ppermute(w, row, near) for w in mine]
    over_w = [lax.ppermute(w, row, over) for w in mine]
    swap_w = [lax.ppermute(w, row, swap) for w in near_w]
    pair_w = [lax.ppermute(w, row, pair) for w in near_w]
    down_w = [lax.ppermute(w, row, down) for w in pair_w]
    shards = [*mine, *over_w, *near_w, *swap_w, *pair_w, *down_w]

    message = dispatch_rows(where, expert_rows, expert_gain.reshape(1, -1), routes, half)
    arrived = lax.all_to_all(
        message.reshape(chips, half, model_width), "ep_0", split_axis=0, concat_axis=0, tiled=True
    )
    outs = expert_rows_out(where, arrived.reshape(chips * half, model_width), shards, chips, n_tp)
    tables = []
    for out in outs:
        back = lax.all_to_all(out, "ep_0", split_axis=0, concat_axis=0, tiled=True)
        table = lax.all_to_all(back, "tp", split_axis=1, concat_axis=1, tiled=True)
        tables.append(table.reshape(EXPERTS * capacity, out.shape[-1]))
    expert_out = combine_rows(*tables, routes.T, route_weight.T, capacity)

    k_normed = head_norm(key_rows, key_gain).astype(jnp.bfloat16)
    kv_own = lax.all_gather(
        jnp.concatenate([k_normed, value_rows], axis=1), "ep_0", axis=0, tiled=False
    )
    cores = [(0, 1), (1, 0)]
    kv_other = lax.ppermute(kv_own, "ep_1", cores)
    attended = attention(where, queries, query_gain.reshape(1, -1), kv_own, kv_other, log_forget)
    own_rows = lax.all_to_all(attended, "tp", split_axis=0, concat_axis=1, tiled=True)
    head_weight = lax.dynamic_slice_in_dim(out_weight, core * HEAD_SIZE, HEAD_SIZE, 0)
    weight_own = lax.all_gather(head_weight, "tp", axis=0, tiled=True)
    weight_other = lax.ppermute(weight_own, "ep_1", cores)
    by_head = own_rows.reshape(own_rows.shape[0], n_tp, CORES, HEAD_SIZE)
    even = by_head[:, :, 0].reshape(own_rows.shape[0], -1)
    odd = by_head[:, :, 1].reshape(own_rows.shape[0], -1)
    projected = jnp.dot(
        jnp.where(core == 0, even, odd), weight_own, preferred_element_type=jnp.float32
    ) + jnp.dot(jnp.where(core == 0, odd, even), weight_other, preferred_element_type=jnp.float32)
    return (projected.astype(jnp.bfloat16), expert_out)


def solution(mesh):
    split = Mesh(
        mesh.devices.reshape(
            mesh.shape["grp"], mesh.shape["ep"] // CORES, CORES, mesh.shape["tp"]
        ),
        ("grp", "ep_0", "ep_1", "tp"),
    )
    in_specs = (
        P(GRP_EP, "tp"),
        P(GRP_EP, "tp"),
        P(GRP_EP, "tp"),
        P(),
        P(),
        P("tp", "grp"),
        P("tp", None),
        P(GRP_EP, None),
        P(),
        P(None, GRP_EP),
        P(None, GRP_EP),
        P(EP, None, "tp"),
        P(EP, None, "tp"),
        P(EP, "tp", None),
    )
    out_specs = (P(GRP_EP_TP, None), P(GRP_EP, "tp"))
    return jax.shard_map(
        on_device, mesh=split, in_specs=in_specs, out_specs=out_specs, check_vma=False
    )
```

```python
import functools

import jax
import jax.numpy as jnp
from jax import lax
from jax.experimental import pallas as pl
from jax.experimental.pallas import tpu as pltpu
from jax.sharding import Mesh
from jax.sharding import PartitionSpec as P

HEAD_SIZE = 128
EXPERTS = 32
TOP = 2
CORES = 2
EP = ("ep_0", "ep_1")
GRP_EP = ("grp", "ep_0", "ep_1")
GRP_EP_TP = ("grp", "ep_0", "ep_1", "tp")
LOG2E = 1.4426950408889634
MIB = 1024 * 1024


SMEM = pl.BlockSpec(memory_space=pltpu.SMEM)
VMEM = pl.BlockSpec(memory_space=pltpu.VMEM)
HBM = pl.BlockSpec(memory_space=pltpu.HBM)


def cost(flops, bytes_accessed, transcendentals=0):
    return pl.CostEstimate(
        flops=int(flops), bytes_accessed=int(bytes_accessed), transcendentals=int(transcendentals)
    )


def params(limit_mib):
    return pltpu.CompilerParams(vmem_limit_bytes=limit_mib * MIB)


def head_norm(inputs, scale_gain):
    widened = inputs.astype(jnp.float32)
    factor = lax.rsqrt(jnp.mean(widened * widened, axis=-1, keepdims=True) + 1e-06)
    return widened * factor * scale_gain


def dispatch_kernel(half, where_ref, rows_ref, gain_ref, routes_ref, out_ref, normed_ref):
    tp_index = where_ref[0]
    n_rows, width = rows_ref.shape
    step = 64

    def norm_step(i, carry):
        part = pl.ds(pl.multiple_of(i * step, step), step)
        normed_ref[part, :] = head_norm(rows_ref[part, :], gain_ref[...]).astype(jnp.bfloat16)
        return carry

    lax.fori_loop(0, n_rows // step, norm_step, 0)
    ids = routes_ref[...]
    expert_iota = lax.broadcasted_iota(jnp.int32, (EXPERTS, n_rows), 0)
    before = jnp.where(
        lax.broadcasted_iota(jnp.int32, (n_rows, n_rows), 0)
        < lax.broadcasted_iota(jnp.int32, (n_rows, n_rows), 1),
        1.0,
        0.0,
    ).astype(jnp.bfloat16)
    base = jnp.zeros((EXPERTS, 1), jnp.float32)
    targets = []
    for j in range(TOP):
        picked = ids[j : j + 1, :]
        one_hot = jnp.where(expert_iota == picked, 1.0, 0.0)
        rank = base + jnp.dot(
            one_hot.astype(jnp.bfloat16), before, preferred_element_type=jnp.float32
        )
        within = jnp.sum(one_hot * rank, axis=0, keepdims=True).astype(jnp.int32)
        base = base + jnp.sum(one_hot, axis=1, keepdims=True)
        low = (tp_index & 1) * half
        mine = ((picked & 1) == (tp_index >> 1)) & (within >= low) & (within < low + half)
        targets.append(jnp.where(mine, (picked >> 1) * half + within - low, -1))
    out_rows = out_ref.shape[0]
    row_iota = lax.broadcasted_iota(jnp.int32, (out_rows, n_rows), 0)
    select = jnp.where((row_iota == targets[0]) | (row_iota == targets[1]), 1.0, 0.0).astype(
        jnp.bfloat16
    )
    span = 512
    for start in range(0, width, span):
        cols = slice(start, start + span)
        out_ref[:, cols] = jnp.dot(
            select, normed_ref[:, cols], preferred_element_type=jnp.float32
        ).astype(jnp.bfloat16)


def dispatch_rows(where, expert_rows, gain, routes, half):
    n_rows, width = expert_rows.shape
    out_rows = EXPERTS // CORES * half
    return pl.pallas_call(
        functools.partial(dispatch_kernel, half),
        out_shape=jax.ShapeDtypeStruct((out_rows, width), jnp.bfloat16),
        in_specs=[SMEM, VMEM, VMEM, VMEM],
        out_specs=VMEM,
        scratch_shapes=[pltpu.VMEM((n_rows, width), jnp.bfloat16)],
        compiler_params=params(24),
        cost_estimate=cost(2 * out_rows * n_rows * width, 2 * (n_rows + out_rows) * width),
        name="dispatch",
    )(where, expert_rows, gain, routes)


def combine_kernel(half, n_tp, where_ref, *refs):
    tables = refs[: 2 * n_tp]
    routes_ref, weight_ref, out_ref = refs[2 * n_tp :]
    tp_index = where_ref[0]
    n_rows = out_ref.shape[0]
    ids = routes_ref[...]
    expert_iota = lax.broadcasted_iota(jnp.int32, (n_rows, EXPERTS), 1)
    before = jnp.where(
        lax.broadcasted_iota(jnp.int32, (n_rows, n_rows), 1)
        < lax.broadcasted_iota(jnp.int32, (n_rows, n_rows), 0),
        1.0,
        0.0,
    ).astype(jnp.bfloat16)
    base = jnp.zeros((1, EXPERTS), jnp.float32)
    table_rows, width = tables[0].shape
    slot_iota = lax.broadcasted_iota(jnp.int32, (n_rows, table_rows), 1)
    selects = []
    for j in range(TOP):
        picked = ids[:, j : j + 1]
        one_hot = jnp.where(expert_iota == picked, 1.0, 0.0)
        rank = base + jnp.dot(
            before, one_hot.astype(jnp.bfloat16), preferred_element_type=jnp.float32
        )
        within = jnp.sum(one_hot * rank, axis=1, keepdims=True).astype(jnp.int32)
        base = base + jnp.sum(one_hot, axis=0, keepdims=True)
        upper = (within >= half).astype(jnp.int32)
        source = (picked & 1) * 2 + upper
        place = (picked >> 1) * half + within - upper * half
        for k in range(n_tp):
            wanted = jnp.where(source == ((tp_index + n_tp - k) & (n_tp - 1)), place, -1)
            selects.append(jnp.where(slot_iota == wanted, 1.0, 0.0).astype(jnp.bfloat16))
    for u in range(2):
        total = jnp.zeros((n_rows, width), jnp.float32)
        for j in range(TOP):
            rows = jnp.zeros((n_rows, width), jnp.float32)
            for k in range(n_tp):
                rows = rows + jnp.dot(
                    selects[j * n_tp + k],
                    tables[u * n_tp + k][...],
                    preferred_element_type=jnp.float32,
                )
            total = total + weight_ref[:, j : j + 1] * rows
        out_ref[:, u * width : (u + 1) * width] = total.astype(jnp.bfloat16)


def combine_rows(where, tables, routes_t, weight_t, half, n_tp):
    n_rows = routes_t.shape[0]
    slots, width = tables[0].shape
    return pl.pallas_call(
        functools.partial(combine_kernel, half, n_tp),
        out_shape=jax.ShapeDtypeStruct((n_rows, 2 * width), jnp.bfloat16),
        in_specs=[SMEM] + [VMEM] * (len(tables) + 2),
        out_specs=VMEM,
        compiler_params=params(32),
        cost_estimate=cost(8 * n_tp * n_rows * slots * width, 4 * n_tp * slots * width),
        name="combine",
    )(where, *tables, routes_t, weight_t)


def expert_kernel(where_ref, x_ref, *refs):
    sources = [refs[3 * i : 3 * i + 3] for i in range(6)]
    outs = refs[18:20]
    gate_buf, up_buf, down_buf, hidden_ref, acc_ref, sems = refs[20:]
    bufs = (gate_buf, up_buf, down_buf)
    core, tp_index = where_ref[1], where_ref[0]
    home = core == (tp_index >> 1)

    def fetch(place, source):
        for i in range(3):
            pltpu.make_async_copy(source[i], bufs[i].at[place], sems.at[place, i]).start()

    pl.when(home)(lambda: fetch(0, sources[0]))
    pl.when(jnp.logical_not(home))(lambda: fetch(0, sources[1]))
    fetch(1, sources[2])
    fetch(2, sources[3])
    pl.when(core == 1)(lambda: fetch(3, sources[4]))
    pl.when(core == 0)(lambda: fetch(3, sources[5]))

    n_rows = x_ref.shape[0]
    depth = acc_ref.shape[1]
    half_rows = n_rows // 2
    acc_ref[...] = jnp.zeros_like(acc_ref)

    def shard(p, carry):
        for i in range(3):
            pltpu.make_async_copy(sources[2][i], bufs[i].at[p], sems.at[p, i]).wait()
        for part in range(2):
            rows = slice(part * half_rows, (part + 1) * half_rows)
            x = x_ref[rows, :]
            gate = jnp.dot(x, gate_buf[p], preferred_element_type=jnp.float32)
            up = jnp.dot(x, up_buf[p], preferred_element_type=jnp.float32)
            hidden_ref[rows, :] = (gate / (1.0 + jnp.exp(-gate)) * up).astype(jnp.bfloat16)
        for start in range(0, depth, 512):
            cols = slice(start, start + 512)
            piece = jnp.dot(
                hidden_ref[...], down_buf[p, :, cols], preferred_element_type=jnp.float32
            )
            acc_ref[:, cols] += piece.astype(jnp.bfloat16).astype(jnp.float32)
        return carry

    lax.fori_loop(0, gate_buf.shape[0], shard, 0)
    chips, n_tp, block, width = outs[0].shape

    def put(chip, carry):
        rows = pl.ds(pl.multiple_of(chip * block, 8), block)
        for u in range(2):
            for k in range(n_tp):
                start = (((tp_index + k) & (n_tp - 1)) * 2 + u) * width
                cols = pl.ds(pl.multiple_of(start, width), width)
                outs[u][chip, k] = acc_ref[rows, cols].astype(jnp.bfloat16)
        return carry

    lax.fori_loop(0, chips, put, 0)


def expert_rows_out(where, x, shards, chips, n_tp):
    n_rows, depth = x.shape
    ff_part = shards[0].shape[1]
    width = depth // n_tp // 2
    out = jax.ShapeDtypeStruct((chips, n_tp, n_rows // chips, width), jnp.bfloat16)
    return pl.pallas_call(
        expert_kernel,
        out_shape=(out, out),
        in_specs=[SMEM, VMEM] + [HBM] * len(shards),
        out_specs=(VMEM, VMEM),
        scratch_shapes=[
            pltpu.VMEM((n_tp, depth, ff_part), jnp.bfloat16),
            pltpu.VMEM((n_tp, depth, ff_part), jnp.bfloat16),
            pltpu.VMEM((n_tp, ff_part, depth), jnp.bfloat16),
            pltpu.VMEM((n_rows, ff_part), jnp.bfloat16),
            pltpu.VMEM((n_rows, depth), jnp.float32),
            pltpu.SemaphoreType.DMA((n_tp, 3)),
        ],
        compiler_params=params(60),
        cost_estimate=cost(
            6 * n_rows * depth * ff_part * n_tp, 6 * n_tp * depth * ff_part + 4 * n_rows * depth
        ),
        name="experts",
    )(where, x, *shards)


def attention_kernel(
    where_ref, q_ref, gain_ref, own_ref, other_ref, gates_ref, out_ref, q_buf, max_ref, acc_ref
):
    chip, core = where_ref[2], where_ref[1]
    span = q_ref.shape[0]
    heads = q_ref.shape[1] // HEAD_SIZE
    scale = HEAD_SIZE ** (-0.5) * LOG2E
    my_block = chip * CORES + core

    def gate_row(r, block):
        return gates_ref[r : r + 1, pl.ds(pl.multiple_of(block * span, span), span)]

    origin = []
    for r in range(heads):
        cols = slice(r * HEAD_SIZE, (r + 1) * HEAD_SIZE)
        q_buf[r] = head_norm(q_ref[:, cols], gain_ref[...]).astype(jnp.bfloat16)
        origin.append(gate_row(r, my_block)[:, 0:1])

    def scores(r, kv_ref, place, block):
        product = lax.dot_general(
            q_buf[r],
            kv_ref[place, :, 0:HEAD_SIZE],
            (((1,), (1,)), ((), ())),
            preferred_element_type=jnp.float32,
        )
        return product * scale + (origin[r] - gate_row(r, block)) * LOG2E

    def weighted(prob, kv_ref, place):
        values = kv_ref[place, :, HEAD_SIZE : 2 * HEAD_SIZE]
        return jnp.dot(
            prob.astype(jnp.bfloat16),
            jnp.concatenate([values, jnp.ones_like(values)], axis=1),
            preferred_element_type=jnp.float32,
        )

    def first(r):
        logits = scores(r, own_ref, chip, my_block)
        row = lax.broadcasted_iota(jnp.int32, (span, span), 0)
        col = lax.broadcasted_iota(jnp.int32, (span, span), 1)
        logits = jnp.where(col <= row, logits, -jnp.inf)
        top = jnp.max(logits, axis=1, keepdims=True)
        prob = jnp.exp2(logits - top)
        max_ref[r] = top
        acc_ref[r] = weighted(prob, own_ref, chip)

    def update(r, parts):
        logits = [scores(r, ref, place, block) for ref, place, block in parts]
        old = max_ref[r]
        top = old
        for part in logits:
            top = jnp.maximum(top, jnp.max(part, axis=1, keepdims=True))
        shrink = jnp.exp2(old - top)
        acc = shrink * acc_ref[r]
        for part, (ref, place, block) in zip(logits, parts):
            prob = jnp.exp2(part - top)
            acc = acc + weighted(prob, ref, place)
        max_ref[r] = top
        acc_ref[r] = acc

    for r in range(heads):
        first(r)

    @pl.when(core == 1)
    def _():
        for r in range(heads):
            update(r, [(other_ref, chip, my_block - 1)])

    def step(place, carry):
        for r in range(heads):
            update(
                r,
                [
                    (own_ref, place, place * CORES + core),
                    (other_ref, place, place * CORES + 1 - core),
                ],
            )
        return carry

    lax.fori_loop(0, chip, step, 0)
    n_tp, part = out_ref.shape[:2]
    for r in range(heads):
        cols = slice(r * HEAD_SIZE, (r + 1) * HEAD_SIZE)
        for k in range(n_tp):
            start = ((where_ref[0] + k) & (n_tp - 1)) * part
            rows = pl.ds(pl.multiple_of(start, part), part)
            out_ref[k, :, cols] = (
                acc_ref[r, rows, :HEAD_SIZE] / acc_ref[r, rows, HEAD_SIZE:]
            ).astype(jnp.bfloat16)


def attention(where, queries, query_gain, kv_own, kv_other, gates, n_tp):
    span, width = queries.shape
    heads = width // HEAD_SIZE
    keys = gates.shape[1]
    return pl.pallas_call(
        attention_kernel,
        out_shape=jax.ShapeDtypeStruct((n_tp, span // n_tp, width), jnp.bfloat16),
        in_specs=[SMEM] + [VMEM] * 5,
        out_specs=VMEM,
        scratch_shapes=[
            pltpu.VMEM((heads, span, HEAD_SIZE), jnp.bfloat16),
            pltpu.VMEM((heads, span, 1), jnp.float32),
            pltpu.VMEM((heads, span, 2 * HEAD_SIZE), jnp.float32),
        ],
        compiler_params=params(40),
        cost_estimate=cost(8 * span * keys * width, 4 * keys * HEAD_SIZE, span * keys * heads),
        name="attention",
    )(where, queries, query_gain, kv_own, kv_other, gates)


def project_kernel(where_ref, *refs):
    pieces, (own_ref, other_ref, out_ref) = refs[:-3], refs[-3:]
    n_tp = len(pieces)
    tp_index, core = where_ref[0], where_ref[1]
    mine = pl.ds(pl.multiple_of(core * HEAD_SIZE, HEAD_SIZE), HEAD_SIZE)
    theirs = pl.ds(pl.multiple_of((1 - core) * HEAD_SIZE, HEAD_SIZE), HEAD_SIZE)
    total = jnp.zeros(out_ref.shape, jnp.float32)
    for k in range(n_tp):
        source = (tp_index + n_tp - k) & (n_tp - 1)
        for cols, weight in ((mine, own_ref), (theirs, other_ref)):
            total = total + jnp.dot(
                pieces[k][:, cols], weight[source], preferred_element_type=jnp.float32
            )
    out_ref[...] = total.astype(jnp.bfloat16)


def project(where, pieces, weight_own, weight_other):
    rows, width = pieces[0].shape
    depth = weight_own.shape[2]
    return pl.pallas_call(
        project_kernel,
        out_shape=jax.ShapeDtypeStruct((rows, depth), jnp.bfloat16),
        in_specs=[SMEM] + [VMEM] * (len(pieces) + 2),
        out_specs=VMEM,
        compiler_params=params(24),
        cost_estimate=cost(
            2 * len(pieces) * rows * width * depth, 2 * len(pieces) * width * depth
        ),
        name="project",
    )(where, *pieces, weight_own, weight_other)


def shard_moves(n_tp):
    at = lambda core, t: core * n_tp + t
    near, over, up = [], [], []
    for core in range(CORES):
        for t in range(n_tp):
            if t // 2 == core:
                near.append((at(core, t), at(0, t ^ 1)))
                over.append((at(core, t), at(1 - core, t)))
            else:
                near.append((at(core, t), at(1, n_tp - 1 - t)))
    swap = [(at(c, t), at(1 - c, t)) for c in range(CORES) for t in range(n_tp)]
    pair = [(at(1, t), at(1, t ^ 1)) for t in range(n_tp)]
    down = [(at(1, t), at(0, t)) for t in range(n_tp)]
    return near, over, swap, pair, down


def on_device(
    queries,
    key_rows,
    value_rows,
    query_gain,
    key_gain,
    log_forget,
    out_weight,
    expert_rows,
    expert_gain,
    routes,
    route_weight,
    gate_weight,
    up_weight,
    down_weight,
):
    n_tp = lax.axis_size("tp")
    chips = lax.axis_size("ep_0")
    chip, core, tp_index = (lax.axis_index(a) for a in ("ep_0", "ep_1", "tp"))
    where = jnp.stack([tp_index, core, chip]).astype(jnp.int32)
    span_rows, model_width = expert_rows.shape
    capacity = n_tp * ((3 * (span_rows // n_tp) * TOP + 2 * EXPERTS - 1) // (2 * EXPERTS))
    half = capacity // 2
    row = ("ep_1", "tp")

    near, over, swap, pair, down = shard_moves(n_tp)
    mine = (gate_weight[0], up_weight[0], down_weight[0])
    near_w = [lax.ppermute(w, row, near) for w in mine]
    over_w = [lax.ppermute(w, row, over) for w in mine]
    swap_w = [lax.ppermute(w, row, swap) for w in near_w]
    pair_w = [lax.ppermute(w, row, pair) for w in near_w]
    down_w = [lax.ppermute(w, row, down) for w in pair_w]
    shards = [*mine, *over_w, *near_w, *swap_w, *pair_w, *down_w]

    message = dispatch_rows(where, expert_rows, expert_gain.reshape(1, -1), routes, half)
    arrived = lax.all_to_all(
        message.reshape(chips, half, model_width), "ep_0", split_axis=0, concat_axis=0, tiled=True
    )
    outs = expert_rows_out(where, arrived.reshape(chips * half, model_width), shards, chips, n_tp)
    def turn(parts):
        return [parts[0]] + [
            lax.ppermute(parts[k], "tp", [(t, (t + k) % n_tp) for t in range(n_tp)])
            for k in range(1, n_tp)
        ]

    def exchange(back):
        rows, width = chips * half, back.shape[-1]
        return turn([back[:, k].reshape(rows, width) for k in range(n_tp)])

    first = lax.all_to_all(outs[0], "ep_0", split_axis=0, concat_axis=0, tiled=True)
    second = lax.all_to_all(outs[1], "ep_0", split_axis=0, concat_axis=0, tiled=True)

    k_normed = head_norm(key_rows, key_gain).astype(jnp.bfloat16)
    kv_own = lax.all_gather(
        jnp.concatenate([k_normed, value_rows], axis=1), "ep_0", axis=0, tiled=False
    )
    cores = [(0, 1), (1, 0)]
    kv_other = lax.ppermute(kv_own, "ep_1", cores)
    first, queries = lax.optimization_barrier((first, queries))
    attended = attention(
        where, queries, query_gain.reshape(1, -1), kv_own, kv_other, log_forget, n_tp
    )
    second, attended = lax.optimization_barrier((second, attended))
    head_weight = lax.dynamic_slice_in_dim(out_weight, core * HEAD_SIZE, HEAD_SIZE, 0)
    weight_own = lax.all_gather(head_weight, "tp", axis=0, tiled=False)
    weight_other = lax.ppermute(weight_own, "ep_1", cores)
    pieces = turn([attended[k] for k in range(n_tp)])
    mixer_out = project(where, pieces, weight_own, weight_other)

    tables = exchange(first) + exchange(second)
    expert_out = combine_rows(where, tables, routes.T, route_weight.T, half, n_tp)
    return (mixer_out, expert_out)


def solution(mesh):
    split = Mesh(
        mesh.devices.reshape(
            mesh.shape["grp"], mesh.shape["ep"] // CORES, CORES, mesh.shape["tp"]
        ),
        ("grp", "ep_0", "ep_1", "tp"),
    )
    in_specs = (
        P(GRP_EP, "tp"),
        P(GRP_EP, "tp"),
        P(GRP_EP, "tp"),
        P(),
        P(),
        P("tp", "grp"),
        P("tp", None),
        P(GRP_EP, None),
        P(),
        P(None, GRP_EP),
        P(None, GRP_EP),
        P(EP, None, "tp"),
        P(EP, None, "tp"),
        P(EP, "tp", None),
    )
    out_specs = (P(GRP_EP_TP, None), P(GRP_EP, "tp"))
    return jax.shard_map(
        on_device, mesh=split, in_specs=in_specs, out_specs=out_specs, check_vma=False
    )
```

```python
import functools

import jax
import jax.numpy as jnp
from jax import lax
from jax.experimental import pallas as pl
from jax.experimental.pallas import tpu as pltpu
from jax.sharding import Mesh
from jax.sharding import PartitionSpec as P

HEAD_SIZE = 128
EXPERTS = 32
TOP = 2
CORES = 2
EP = ("ep_0", "ep_1")
GRP_EP = ("grp", "ep_0", "ep_1")
GRP_EP_TP = ("grp", "ep_0", "ep_1", "tp")
LOG2E = 1.4426950408889634
MIB = 1024 * 1024


SMEM = pl.BlockSpec(memory_space=pltpu.SMEM)
VMEM = pl.BlockSpec(memory_space=pltpu.VMEM)
HBM = pl.BlockSpec(memory_space=pltpu.HBM)


def cost(flops, bytes_accessed, transcendentals=0):
    return pl.CostEstimate(
        flops=int(flops), bytes_accessed=int(bytes_accessed), transcendentals=int(transcendentals)
    )


def params(limit_mib):
    return pltpu.CompilerParams(vmem_limit_bytes=limit_mib * MIB)


def head_norm(inputs, scale_gain):
    widened = inputs.astype(jnp.float32)
    factor = lax.rsqrt(jnp.mean(widened * widened, axis=-1, keepdims=True) + 1e-06)
    return widened * factor * scale_gain


def dispatch_kernel(half, where_ref, rows_ref, gain_ref, routes_ref, out_ref, normed_ref):
    tp_index = where_ref[0]
    n_rows, width = rows_ref.shape
    step = 64

    def norm_step(i, carry):
        part = pl.ds(pl.multiple_of(i * step, step), step)
        normed_ref[part, :] = head_norm(rows_ref[part, :], gain_ref[...]).astype(jnp.bfloat16)
        return carry

    lax.fori_loop(0, n_rows // step, norm_step, 0)
    ids = routes_ref[...]
    expert_iota = lax.broadcasted_iota(jnp.int32, (EXPERTS, n_rows), 0)
    before = jnp.where(
        lax.broadcasted_iota(jnp.int32, (n_rows, n_rows), 0)
        < lax.broadcasted_iota(jnp.int32, (n_rows, n_rows), 1),
        1.0,
        0.0,
    ).astype(jnp.bfloat16)
    base = jnp.zeros((EXPERTS, 1), jnp.float32)
    targets = []
    for j in range(TOP):
        picked = ids[j : j + 1, :]
        one_hot = jnp.where(expert_iota == picked, 1.0, 0.0)
        rank = base + jnp.dot(
            one_hot.astype(jnp.bfloat16), before, preferred_element_type=jnp.float32
        )
        within = jnp.sum(one_hot * rank, axis=0, keepdims=True).astype(jnp.int32)
        base = base + jnp.sum(one_hot, axis=1, keepdims=True)
        low = (tp_index & 1) * half
        mine = ((picked & 1) == (tp_index >> 1)) & (within >= low) & (within < low + half)
        targets.append(jnp.where(mine, (picked >> 1) * half + within - low, -1))
    out_rows = out_ref.shape[0]
    row_iota = lax.broadcasted_iota(jnp.int32, (out_rows, n_rows), 0)
    select = jnp.where((row_iota == targets[0]) | (row_iota == targets[1]), 1.0, 0.0).astype(
        jnp.bfloat16
    )
    span = 512
    for start in range(0, width, span):
        cols = slice(start, start + span)
        out_ref[:, cols] = jnp.dot(
            select, normed_ref[:, cols], preferred_element_type=jnp.float32
        ).astype(jnp.bfloat16)


def dispatch_rows(where, expert_rows, gain, routes, half):
    n_rows, width = expert_rows.shape
    out_rows = EXPERTS // CORES * half
    return pl.pallas_call(
        functools.partial(dispatch_kernel, half),
        out_shape=jax.ShapeDtypeStruct((out_rows, width), jnp.bfloat16),
        in_specs=[SMEM, VMEM, VMEM, VMEM],
        out_specs=VMEM,
        scratch_shapes=[pltpu.VMEM((n_rows, width), jnp.bfloat16)],
        compiler_params=params(24),
        cost_estimate=cost(2 * out_rows * n_rows * width, 2 * (n_rows + out_rows) * width),
        name="dispatch",
    )(where, expert_rows, gain, routes)


def combine_kernel(half, n_tp, where_ref, *refs):
    tables = refs[:2]
    routes_ref, weight_ref, out_ref = refs[2:]
    tp_index = where_ref[0]
    n_rows = out_ref.shape[0]
    ids = routes_ref[...]
    expert_iota = lax.broadcasted_iota(jnp.int32, (n_rows, EXPERTS), 1)
    before = jnp.where(
        lax.broadcasted_iota(jnp.int32, (n_rows, n_rows), 1)
        < lax.broadcasted_iota(jnp.int32, (n_rows, n_rows), 0),
        1.0,
        0.0,
    ).astype(jnp.bfloat16)
    base = jnp.zeros((1, EXPERTS), jnp.float32)
    table_rows, width = tables[0].shape
    slot_iota = lax.broadcasted_iota(jnp.int32, (n_rows, table_rows), 1)
    selects = []
    for j in range(TOP):
        picked = ids[:, j : j + 1]
        one_hot = jnp.where(expert_iota == picked, 1.0, 0.0)
        rank = base + jnp.dot(
            before, one_hot.astype(jnp.bfloat16), preferred_element_type=jnp.float32
        )
        within = jnp.sum(one_hot * rank, axis=1, keepdims=True).astype(jnp.int32)
        base = base + jnp.sum(one_hot, axis=0, keepdims=True)
        upper = (within >= half).astype(jnp.int32)
        source = (picked & 1) * 2 + upper
        turn = (tp_index + n_tp - source) & (n_tp - 1)
        place = ((picked >> 1) * n_tp + turn) * half + within - upper * half
        selects.append(jnp.where(slot_iota == place, 1.0, 0.0).astype(jnp.bfloat16))
    for u, table in enumerate(tables):
        total = jnp.zeros((n_rows, width), jnp.float32)
        for j in range(TOP):
            rows = jnp.dot(selects[j], table[...], preferred_element_type=jnp.float32)
            total = total + weight_ref[:, j : j + 1] * rows
        out_ref[:, u * width : (u + 1) * width] = total.astype(jnp.bfloat16)


def combine_rows(where, tables, routes_t, weight_t, half, n_tp):
    n_rows = routes_t.shape[0]
    slots, width = tables[0].shape
    return pl.pallas_call(
        functools.partial(combine_kernel, half, n_tp),
        out_shape=jax.ShapeDtypeStruct((n_rows, 2 * width), jnp.bfloat16),
        in_specs=[SMEM] + [VMEM] * (len(tables) + 2),
        out_specs=VMEM,
        compiler_params=params(32),
        cost_estimate=cost(8 * n_rows * slots * width, 4 * slots * width),
        name="combine",
    )(where, *tables, routes_t, weight_t)


def expert_kernel(where_ref, x_ref, *refs):
    sources = [refs[3 * i : 3 * i + 3] for i in range(6)]
    outs = refs[18:-6]
    gate_buf, up_buf, down_buf, hidden_ref, acc_ref, sems = refs[-6:]
    bufs = (gate_buf, up_buf, down_buf)
    core, tp_index = where_ref[1], where_ref[0]
    home = core == (tp_index >> 1)

    def fetch(place, source):
        for i in range(3):
            pltpu.make_async_copy(source[i], bufs[i].at[place], sems.at[place, i]).start()

    pl.when(home)(lambda: fetch(0, sources[0]))
    pl.when(jnp.logical_not(home))(lambda: fetch(0, sources[1]))
    fetch(1, sources[2])
    fetch(2, sources[3])
    pl.when(core == 1)(lambda: fetch(3, sources[4]))
    pl.when(core == 0)(lambda: fetch(3, sources[5]))

    n_rows = x_ref.shape[0]
    depth = acc_ref.shape[1]
    half_rows = n_rows // 2
    acc_ref[...] = jnp.zeros_like(acc_ref)

    def shard(p, carry):
        for i in range(3):
            pltpu.make_async_copy(sources[2][i], bufs[i].at[p], sems.at[p, i]).wait()
        for part in range(2):
            rows = slice(part * half_rows, (part + 1) * half_rows)
            x = x_ref[rows, :]
            gate = jnp.dot(x, gate_buf[p], preferred_element_type=jnp.float32)
            up = jnp.dot(x, up_buf[p], preferred_element_type=jnp.float32)
            hidden_ref[rows, :] = (gate / (1.0 + jnp.exp(-gate)) * up).astype(jnp.bfloat16)
        for start in range(0, depth, 512):
            cols = slice(start, start + 512)
            piece = jnp.dot(
                hidden_ref[...], down_buf[p, :, cols], preferred_element_type=jnp.float32
            )
            acc_ref[:, cols] += piece.astype(jnp.bfloat16).astype(jnp.float32)
        return carry

    lax.fori_loop(0, gate_buf.shape[0], shard, 0)
    n_tp = gate_buf.shape[0]
    width = outs[0].shape[1]
    for u in range(2):
        for k in range(n_tp):
            start = (((tp_index + k) & (n_tp - 1)) * 2 + u) * width
            cols = pl.ds(pl.multiple_of(start, width), width)
            outs[u * n_tp + k][...] = acc_ref[:, cols].astype(jnp.bfloat16)


def expert_rows_out(where, x, shards, n_tp):
    n_rows, depth = x.shape
    ff_part = shards[0].shape[1]
    width = depth // n_tp // 2
    out = jax.ShapeDtypeStruct((n_rows, width), jnp.bfloat16)
    return pl.pallas_call(
        expert_kernel,
        out_shape=[out] * (2 * n_tp),
        in_specs=[SMEM, VMEM] + [HBM] * len(shards),
        out_specs=[VMEM] * (2 * n_tp),
        scratch_shapes=[
            pltpu.VMEM((n_tp, depth, ff_part), jnp.bfloat16),
            pltpu.VMEM((n_tp, depth, ff_part), jnp.bfloat16),
            pltpu.VMEM((n_tp, ff_part, depth), jnp.bfloat16),
            pltpu.VMEM((n_rows, ff_part), jnp.bfloat16),
            pltpu.VMEM((n_rows, depth), jnp.float32),
            pltpu.SemaphoreType.DMA((n_tp, 3)),
        ],
        compiler_params=params(60),
        cost_estimate=cost(
            6 * n_rows * depth * ff_part * n_tp, 6 * n_tp * depth * ff_part + 4 * n_rows * depth
        ),
        name="experts",
    )(where, x, *shards)


def attention_kernel(
    where_ref, q_ref, gain_ref, own_ref, other_ref, gates_ref, out_ref, q_buf, max_ref, acc_ref, logit_ref
):
    chip, core = where_ref[2], where_ref[1]
    span = q_ref.shape[0]
    heads = q_ref.shape[1] // HEAD_SIZE
    scale = HEAD_SIZE ** (-0.5) * LOG2E
    my_block = chip * CORES + core

    def gate_row(r, block):
        return gates_ref[r : r + 1, pl.ds(pl.multiple_of(block * span, span), span)]

    origin = []
    for r in range(heads):
        cols = slice(r * HEAD_SIZE, (r + 1) * HEAD_SIZE)
        q_buf[r] = head_norm(q_ref[:, cols], gain_ref[...]).astype(jnp.bfloat16)
        origin.append(gate_row(r, my_block)[:, 0:1])

    def scores(r, kv_ref, place, block):
        product = lax.dot_general(
            q_buf[r],
            kv_ref[place, :, 0:HEAD_SIZE],
            (((1,), (1,)), ((), ())),
            preferred_element_type=jnp.float32,
        )
        return product * scale + (origin[r] - gate_row(r, block)) * LOG2E

    def weighted(prob, kv_ref, place):
        values = kv_ref[place, :, HEAD_SIZE : 2 * HEAD_SIZE]
        return jnp.dot(
            prob.astype(jnp.bfloat16),
            jnp.concatenate([values, jnp.ones_like(values)], axis=1),
            preferred_element_type=jnp.float32,
        )

    def first(r):
        logits = scores(r, own_ref, chip, my_block)
        row = lax.broadcasted_iota(jnp.int32, (span, span), 0)
        col = lax.broadcasted_iota(jnp.int32, (span, span), 1)
        logits = jnp.where(col <= row, logits, -jnp.inf)
        top = jnp.max(logits, axis=1, keepdims=True)
        prob = jnp.exp2(logits - top)
        max_ref[r] = top
        acc_ref[r] = weighted(prob, own_ref, chip)

    def fill(r, place):
        for i, ref in enumerate((own_ref, other_ref)):
            block = place * CORES + (core if i == 0 else 1 - core)
            logit_ref[r, :, i * span : (i + 1) * span] = scores(r, ref, place, block)

    def absorb(r, logits, pieces):
        old = max_ref[r]
        top = jnp.maximum(old, jnp.max(logits, axis=1, keepdims=True))
        acc = jnp.exp2(old - top) * acc_ref[r]
        max_ref[r] = top
        prob = jnp.exp2(logits - top)
        for i, (ref, place) in enumerate(pieces):
            acc = acc + weighted(prob[:, i * span : (i + 1) * span], ref, place)
        acc_ref[r] = acc

    for r in range(heads):
        first(r)

    @pl.when(core == 1)
    def _():
        for r in range(heads):
            absorb(r, scores(r, other_ref, chip, my_block - 1), [(other_ref, chip)])

    fill(0, 0)

    def step(place, carry):
        pieces = [(own_ref, place), (other_ref, place)]
        for r in range(heads):
            if r + 1 < heads:
                fill(r + 1, place)
            absorb(r, logit_ref[r], pieces)
            if r + 1 == heads - 1:
                fill(0, jnp.minimum(place + 1, chip))
        return carry

    lax.fori_loop(0, chip, step, 0)
    n_tp, part = out_ref.shape[:2]
    for r in range(heads):
        cols = slice(r * HEAD_SIZE, (r + 1) * HEAD_SIZE)
        for k in range(n_tp):
            start = ((where_ref[0] + k) & (n_tp - 1)) * part
            rows = pl.ds(pl.multiple_of(start, part), part)
            out_ref[k, :, cols] = (
                acc_ref[r, rows, :HEAD_SIZE] / acc_ref[r, rows, HEAD_SIZE:]
            ).astype(jnp.bfloat16)


def attention(where, queries, query_gain, kv_own, kv_other, gates, n_tp):
    span, width = queries.shape
    heads = width // HEAD_SIZE
    keys = gates.shape[1]
    return pl.pallas_call(
        attention_kernel,
        out_shape=jax.ShapeDtypeStruct((n_tp, span // n_tp, width), jnp.bfloat16),
        in_specs=[SMEM] + [VMEM] * 5,
        out_specs=VMEM,
        scratch_shapes=[
            pltpu.VMEM((heads, span, HEAD_SIZE), jnp.bfloat16),
            pltpu.VMEM((heads, span, 1), jnp.float32),
            pltpu.VMEM((heads, span, 2 * HEAD_SIZE), jnp.float32),
            pltpu.VMEM((heads, span, CORES * span), jnp.float32),
        ],
        compiler_params=params(40),
        cost_estimate=cost(8 * span * keys * width, 4 * keys * HEAD_SIZE, span * keys * heads),
        name="attention",
    )(where, queries, query_gain, kv_own, kv_other, gates)


def project_kernel(*refs):
    out_ref = refs[-1]
    n_tp = len(refs) // 2
    total = jnp.zeros(out_ref.shape, jnp.float32)
    for piece, weight in zip(refs[:n_tp], refs[n_tp:-1]):
        total = total + jnp.dot(piece[...], weight[...], preferred_element_type=jnp.float32)
    out_ref[...] = total.astype(jnp.bfloat16)


def project(pieces, weights):
    rows, width = pieces[0].shape
    depth = weights[0].shape[1]
    return pl.pallas_call(
        project_kernel,
        out_shape=jax.ShapeDtypeStruct((rows, depth), jnp.bfloat16),
        in_specs=[VMEM] * (len(pieces) + len(weights)),
        out_specs=VMEM,
        compiler_params=params(24),
        cost_estimate=cost(
            2 * len(pieces) * rows * width * depth, 2 * len(pieces) * width * depth
        ),
        name="project",
    )(*pieces, *weights)


def shard_moves(n_tp):
    at = lambda core, t: core * n_tp + t
    near, over, up = [], [], []
    for core in range(CORES):
        for t in range(n_tp):
            if t // 2 == core:
                near.append((at(core, t), at(0, t ^ 1)))
                over.append((at(core, t), at(1 - core, t)))
            else:
                near.append((at(core, t), at(1, n_tp - 1 - t)))
    swap = [(at(c, t), at(1 - c, t)) for c in range(CORES) for t in range(n_tp)]
    pair = [(at(1, t), at(1, t ^ 1)) for t in range(n_tp)]
    down = [(at(1, t), at(0, t)) for t in range(n_tp)]
    return near, over, swap, pair, down


def on_device(
    queries,
    key_rows,
    value_rows,
    query_gain,
    key_gain,
    log_forget,
    out_weight,
    expert_rows,
    expert_gain,
    routes,
    route_weight,
    gate_weight,
    up_weight,
    down_weight,
):
    n_tp = lax.axis_size("tp")
    chips = lax.axis_size("ep_0")
    chip, core, tp_index = (lax.axis_index(a) for a in ("ep_0", "ep_1", "tp"))
    where = jnp.stack([tp_index, core, chip]).astype(jnp.int32)
    span_rows, model_width = expert_rows.shape
    capacity = n_tp * ((3 * (span_rows // n_tp) * TOP + 2 * EXPERTS - 1) // (2 * EXPERTS))
    half = capacity // 2
    row = ("ep_1", "tp")

    near, over, swap, pair, down = shard_moves(n_tp)
    mine = (gate_weight[0], up_weight[0], down_weight[0])
    near_w = [lax.ppermute(w, row, near) for w in mine]
    over_w = [lax.ppermute(w, row, over) for w in mine]
    swap_w = [lax.ppermute(w, row, swap) for w in near_w]
    pair_w = [lax.ppermute(w, row, pair) for w in near_w]
    down_w = [lax.ppermute(w, row, down) for w in pair_w]
    shards = [*mine, *over_w, *near_w, *swap_w, *pair_w, *down_w]

    message = dispatch_rows(where, expert_rows, expert_gain.reshape(1, -1), routes, half)
    arrived = lax.all_to_all(
        message.reshape(chips, half, model_width), "ep_0", split_axis=0, concat_axis=0, tiled=True
    )
    arrived, out_weight = lax.optimization_barrier((arrived, out_weight))
    outs = expert_rows_out(where, arrived.reshape(chips * half, model_width), shards, n_tp)

    def turn(parts):
        return [parts[0]] + [
            lax.ppermute(parts[k], "tp", [(t, (t + k) % n_tp) for t in range(n_tp)])
            for k in range(1, n_tp)
        ]

    def joined(parts):
        return jnp.stack([part.reshape(chips, half, part.shape[1]) for part in turn(parts)], axis=1)

    def send_back(table):
        return lax.all_to_all(table, "ep_0", split_axis=0, concat_axis=0, tiled=True)

    first = send_back(joined(outs[:n_tp]))
    second = joined(outs[n_tp:])

    k_normed = head_norm(key_rows, key_gain).astype(jnp.bfloat16)
    kv_own = lax.all_gather(
        jnp.concatenate([k_normed, value_rows], axis=1), "ep_0", axis=0, tiled=False
    )
    first, second, queries, kv_own = lax.optimization_barrier((first, second, queries, kv_own))
    second = send_back(second)
    kv_other = lax.ppermute(kv_own, "ep_1", [(0, 1), (1, 0)])
    attended = attention(
        where, queries, query_gain.reshape(1, -1), kv_own, kv_other, log_forget, n_tp
    )
    pieces = turn([attended[k] for k in range(n_tp)])
    weights = turn([out_weight] * n_tp)
    mixer_out = project(pieces, weights)
    second, mixer_out = lax.optimization_barrier((second, mixer_out))

    tables = [part.reshape(EXPERTS * capacity, part.shape[-1]) for part in (first, second)]
    expert_out = combine_rows(where, tables, routes.T, route_weight.T, half, n_tp)
    return (mixer_out, expert_out)


def solution(mesh):
    split = Mesh(
        mesh.devices.reshape(
            mesh.shape["grp"], mesh.shape["ep"] // CORES, CORES, mesh.shape["tp"]
        ),
        ("grp", "ep_0", "ep_1", "tp"),
    )
    in_specs = (
        P(GRP_EP, "tp"),
        P(GRP_EP, "tp"),
        P(GRP_EP, "tp"),
        P(),
        P(),
        P("tp", "grp"),
        P("tp", None),
        P(GRP_EP, None),
        P(),
        P(None, GRP_EP),
        P(None, GRP_EP),
        P(EP, None, "tp"),
        P(EP, None, "tp"),
        P(EP, "tp", None),
    )
    out_specs = (P(GRP_EP_TP, None), P(GRP_EP, "tp"))
    return jax.shard_map(
        on_device, mesh=split, in_specs=in_specs, out_specs=out_specs, check_vma=False
    )
```

```python
import functools

import jax
import jax.numpy as jnp
from jax import lax
from jax.experimental import pallas as pl
from jax.experimental.pallas import tpu as pltpu
from jax.sharding import Mesh
from jax.sharding import PartitionSpec as P

HEAD_SIZE = 128
EXPERTS = 32
TOP = 2
CORES = 2
EP = ("ep_0", "ep_1")
GRP_EP = ("grp", "ep_0", "ep_1")
GRP_EP_TP = ("grp", "ep_0", "ep_1", "tp")
LOG2E = 1.4426950408889634
MIB = 1024 * 1024


SMEM = pl.BlockSpec(memory_space=pltpu.SMEM)
VMEM = pl.BlockSpec(memory_space=pltpu.VMEM)
HBM = pl.BlockSpec(memory_space=pltpu.HBM)


def cost(flops, bytes_accessed, transcendentals=0):
    return pl.CostEstimate(
        flops=int(flops), bytes_accessed=int(bytes_accessed), transcendentals=int(transcendentals)
    )


def params(limit_mib):
    return pltpu.CompilerParams(vmem_limit_bytes=limit_mib * MIB)


def head_norm(inputs, scale_gain):
    widened = inputs.astype(jnp.float32)
    factor = lax.rsqrt(jnp.mean(widened * widened, axis=-1, keepdims=True) + 1e-06)
    return widened * factor * scale_gain


def dispatch_kernel(half, where_ref, rows_ref, gain_ref, routes_ref, out_ref, normed_ref):
    tp_index = where_ref[0]
    n_rows, width = rows_ref.shape
    step = 64

    def norm_step(i, carry):
        part = pl.ds(pl.multiple_of(i * step, step), step)
        normed_ref[part, :] = head_norm(rows_ref[part, :], gain_ref[...]).astype(jnp.bfloat16)
        return carry

    lax.fori_loop(0, n_rows // step, norm_step, 0)
    ids = routes_ref[...]
    expert_iota = lax.broadcasted_iota(jnp.int32, (EXPERTS, n_rows), 0)
    before = jnp.where(
        lax.broadcasted_iota(jnp.int32, (n_rows, n_rows), 0)
        < lax.broadcasted_iota(jnp.int32, (n_rows, n_rows), 1),
        1.0,
        0.0,
    ).astype(jnp.bfloat16)
    base = jnp.zeros((EXPERTS, 1), jnp.float32)
    targets = []
    for j in range(TOP):
        picked = ids[j : j + 1, :]
        one_hot = jnp.where(expert_iota == picked, 1.0, 0.0)
        rank = base + jnp.dot(
            one_hot.astype(jnp.bfloat16), before, preferred_element_type=jnp.float32
        )
        within = jnp.sum(one_hot * rank, axis=0, keepdims=True).astype(jnp.int32)
        base = base + jnp.sum(one_hot, axis=1, keepdims=True)
        low = (tp_index & 1) * half
        mine = ((picked & 1) == (tp_index >> 1)) & (within >= low) & (within < low + half)
        targets.append(jnp.where(mine, (picked >> 1) * half + within - low, -1))
    out_rows = out_ref.shape[0]
    row_iota = lax.broadcasted_iota(jnp.int32, (out_rows, n_rows), 0)
    select = jnp.where((row_iota == targets[0]) | (row_iota == targets[1]), 1.0, 0.0).astype(
        jnp.bfloat16
    )
    span = 512
    for start in range(0, width, span):
        cols = slice(start, start + span)
        out_ref[:, cols] = jnp.dot(
            select, normed_ref[:, cols], preferred_element_type=jnp.float32
        ).astype(jnp.bfloat16)


def dispatch_rows(where, expert_rows, gain, routes, half):
    n_rows, width = expert_rows.shape
    out_rows = EXPERTS // CORES * half
    return pl.pallas_call(
        functools.partial(dispatch_kernel, half),
        out_shape=jax.ShapeDtypeStruct((out_rows, width), jnp.bfloat16),
        in_specs=[SMEM, VMEM, VMEM, VMEM],
        out_specs=VMEM,
        scratch_shapes=[pltpu.VMEM((n_rows, width), jnp.bfloat16)],
        compiler_params=params(60),
        cost_estimate=cost(2 * out_rows * n_rows * width, 2 * (n_rows + out_rows) * width),
        name="dispatch",
    )(where, expert_rows, gain, routes)


def combine_kernel(half, n_tp, where_ref, *refs):
    tables = refs[:2]
    routes_ref, weight_ref, out_ref = refs[2:]
    tp_index = where_ref[0]
    n_rows = out_ref.shape[0]
    ids = routes_ref[...]
    expert_iota = lax.broadcasted_iota(jnp.int32, (n_rows, EXPERTS), 1)
    before = jnp.where(
        lax.broadcasted_iota(jnp.int32, (n_rows, n_rows), 1)
        < lax.broadcasted_iota(jnp.int32, (n_rows, n_rows), 0),
        1.0,
        0.0,
    ).astype(jnp.bfloat16)
    base = jnp.zeros((1, EXPERTS), jnp.float32)
    table_rows, width = tables[0].shape
    slot_iota = lax.broadcasted_iota(jnp.int32, (n_rows, table_rows), 1)
    selects = []
    for j in range(TOP):
        picked = ids[:, j : j + 1]
        one_hot = jnp.where(expert_iota == picked, 1.0, 0.0)
        rank = base + jnp.dot(
            before, one_hot.astype(jnp.bfloat16), preferred_element_type=jnp.float32
        )
        within = jnp.sum(one_hot * rank, axis=1, keepdims=True).astype(jnp.int32)
        base = base + jnp.sum(one_hot, axis=0, keepdims=True)
        upper = (within >= half).astype(jnp.int32)
        source = (picked & 1) * 2 + upper
        turn = (tp_index + n_tp - source) & (n_tp - 1)
        place = ((picked >> 1) * n_tp + turn) * half + within - upper * half
        selects.append(jnp.where(slot_iota == place, 1.0, 0.0).astype(jnp.bfloat16))
    for u, table in enumerate(tables):
        total = jnp.zeros((n_rows, width), jnp.float32)
        for j in range(TOP):
            rows = jnp.dot(selects[j], table[...], preferred_element_type=jnp.float32)
            total = total + weight_ref[:, j : j + 1] * rows
        out_ref[:, u * width : (u + 1) * width] = total.astype(jnp.bfloat16)


def combine_rows(where, tables, routes_t, weight_t, half, n_tp):
    n_rows = routes_t.shape[0]
    slots, width = tables[0].shape
    return pl.pallas_call(
        functools.partial(combine_kernel, half, n_tp),
        out_shape=jax.ShapeDtypeStruct((n_rows, 2 * width), jnp.bfloat16),
        in_specs=[SMEM] + [VMEM] * (len(tables) + 2),
        out_specs=VMEM,
        compiler_params=params(32),
        cost_estimate=cost(8 * n_rows * slots * width, 4 * slots * width),
        name="combine",
    )(where, *tables, routes_t, weight_t)


def expert_kernel(where_ref, x_ref, *refs):
    sources = [refs[3 * i : 3 * i + 3] for i in range(6)]
    outs = refs[18:-6]
    gate_buf, up_buf, down_buf, hidden_ref, acc_ref, sems = refs[-6:]
    bufs = (gate_buf, up_buf, down_buf)
    core, tp_index = where_ref[1], where_ref[0]
    home = core == (tp_index >> 1)

    def fetch(place, source):
        for i in range(3):
            pltpu.make_async_copy(source[i], bufs[i].at[place], sems.at[place, i]).start()

    pl.when(home)(lambda: fetch(0, sources[0]))
    pl.when(jnp.logical_not(home))(lambda: fetch(0, sources[1]))
    fetch(1, sources[2])
    fetch(2, sources[3])
    pl.when(core == 1)(lambda: fetch(3, sources[4]))
    pl.when(core == 0)(lambda: fetch(3, sources[5]))

    n_rows = x_ref.shape[0]
    depth = acc_ref.shape[1]
    half_rows = n_rows // 2
    acc_ref[...] = jnp.zeros_like(acc_ref)

    def shard(p, carry):
        for i in range(3):
            pltpu.make_async_copy(sources[2][i], bufs[i].at[p], sems.at[p, i]).wait()
        for part in range(2):
            rows = slice(part * half_rows, (part + 1) * half_rows)
            x = x_ref[rows, :]
            gate = jnp.dot(x, gate_buf[p], preferred_element_type=jnp.float32)
            up = jnp.dot(x, up_buf[p], preferred_element_type=jnp.float32)
            hidden_ref[rows, :] = (gate / (1.0 + jnp.exp(-gate)) * up).astype(jnp.bfloat16)
        for start in range(0, depth, 512):
            cols = slice(start, start + 512)
            piece = jnp.dot(
                hidden_ref[...], down_buf[p, :, cols], preferred_element_type=jnp.float32
            )
            acc_ref[:, cols] += piece.astype(jnp.bfloat16).astype(jnp.float32)
        return carry

    lax.fori_loop(0, gate_buf.shape[0], shard, 0)
    n_tp = gate_buf.shape[0]
    width = outs[0].shape[1]
    for u in range(2):
        for k in range(n_tp):
            start = (((tp_index + k) & (n_tp - 1)) * 2 + u) * width
            cols = pl.ds(pl.multiple_of(start, width), width)
            outs[u * n_tp + k][...] = acc_ref[:, cols].astype(jnp.bfloat16)


def expert_rows_out(where, x, shards, n_tp):
    n_rows, depth = x.shape
    ff_part = shards[0].shape[1]
    width = depth // n_tp // 2
    out = jax.ShapeDtypeStruct((n_rows, width), jnp.bfloat16)
    return pl.pallas_call(
        expert_kernel,
        out_shape=[out] * (2 * n_tp),
        in_specs=[SMEM, VMEM] + [HBM] * len(shards),
        out_specs=[VMEM] * (2 * n_tp),
        scratch_shapes=[
            pltpu.VMEM((n_tp, depth, ff_part), jnp.bfloat16),
            pltpu.VMEM((n_tp, depth, ff_part), jnp.bfloat16),
            pltpu.VMEM((n_tp, ff_part, depth), jnp.bfloat16),
            pltpu.VMEM((n_rows, ff_part), jnp.bfloat16),
            pltpu.VMEM((n_rows, depth), jnp.float32),
            pltpu.SemaphoreType.DMA((n_tp, 3)),
        ],
        compiler_params=params(60),
        cost_estimate=cost(
            6 * n_rows * depth * ff_part * n_tp, 6 * n_tp * depth * ff_part + 4 * n_rows * depth
        ),
        name="experts",
    )(where, x, *shards)


def attention_kernel(
    where_ref, q_ref, gain_ref, own_ref, other_ref, gates_ref, out_ref, q_buf, max_ref, acc_ref, logit_ref
):
    chip, core = where_ref[2], where_ref[1]
    span = q_ref.shape[0]
    heads = q_ref.shape[1] // HEAD_SIZE
    scale = HEAD_SIZE ** (-0.5) * LOG2E
    my_block = chip * CORES + core

    def gate_row(r, block):
        return gates_ref[r : r + 1, pl.ds(pl.multiple_of(block * span, span), span)]

    origin = []
    for r in range(heads):
        cols = slice(r * HEAD_SIZE, (r + 1) * HEAD_SIZE)
        q_buf[r] = head_norm(q_ref[:, cols], gain_ref[...]).astype(jnp.bfloat16)
        origin.append(gate_row(r, my_block)[:, 0:1])

    def scores(r, kv_ref, place, block):
        product = lax.dot_general(
            q_buf[r],
            kv_ref[place, :, 0:HEAD_SIZE],
            (((1,), (1,)), ((), ())),
            preferred_element_type=jnp.float32,
        )
        return product * scale + (origin[r] - gate_row(r, block)) * LOG2E

    def weighted(prob, kv_ref, place):
        values = kv_ref[place, :, HEAD_SIZE : 2 * HEAD_SIZE]
        return jnp.dot(
            prob.astype(jnp.bfloat16),
            jnp.concatenate([values, jnp.ones_like(values)], axis=1),
            preferred_element_type=jnp.float32,
        )

    def first(r):
        logits = scores(r, own_ref, chip, my_block)
        row = lax.broadcasted_iota(jnp.int32, (span, span), 0)
        col = lax.broadcasted_iota(jnp.int32, (span, span), 1)
        logits = jnp.where(col <= row, logits, -jnp.inf)
        top = jnp.max(logits, axis=1, keepdims=True)
        prob = jnp.exp2(logits - top)
        max_ref[r] = top
        acc_ref[r] = weighted(prob, own_ref, chip)

    def fill(r, place):
        for i, ref in enumerate((own_ref, other_ref)):
            block = place * CORES + (core if i == 0 else 1 - core)
            logit_ref[r, :, i * span : (i + 1) * span] = scores(r, ref, place, block)

    def absorb(r, logits, pieces):
        old = max_ref[r]
        top = jnp.maximum(old, jnp.max(logits, axis=1, keepdims=True))
        acc = jnp.exp2(old - top) * acc_ref[r]
        max_ref[r] = top
        prob = jnp.exp2(logits - top)
        for i, (ref, place) in enumerate(pieces):
            acc = acc + weighted(prob[:, i * span : (i + 1) * span], ref, place)
        acc_ref[r] = acc

    for r in range(heads):
        first(r)

    @pl.when(core == 1)
    def _():
        for r in range(heads):
            absorb(r, scores(r, other_ref, chip, my_block - 1), [(other_ref, chip)])

    fill(0, 0)

    def step(place, carry):
        pieces = [(own_ref, place), (other_ref, place)]
        for r in range(heads):
            if r + 1 < heads:
                fill(r + 1, place)
            absorb(r, logit_ref[r], pieces)
            if r + 1 == heads - 1:
                fill(0, jnp.minimum(place + 1, chip))
        return carry

    lax.fori_loop(0, chip, step, 0)
    n_tp, part = out_ref.shape[:2]
    for r in range(heads):
        cols = slice(r * HEAD_SIZE, (r + 1) * HEAD_SIZE)
        for k in range(n_tp):
            start = ((where_ref[0] + k) & (n_tp - 1)) * part
            rows = pl.ds(pl.multiple_of(start, part), part)
            out_ref[k, :, cols] = (
                acc_ref[r, rows, :HEAD_SIZE] / acc_ref[r, rows, HEAD_SIZE:]
            ).astype(jnp.bfloat16)


def attention(where, queries, query_gain, kv_own, kv_other, gates, n_tp):
    span, width = queries.shape
    heads = width // HEAD_SIZE
    keys = gates.shape[1]
    return pl.pallas_call(
        attention_kernel,
        out_shape=jax.ShapeDtypeStruct((n_tp, span // n_tp, width), jnp.bfloat16),
        in_specs=[SMEM] + [VMEM] * 5,
        out_specs=VMEM,
        scratch_shapes=[
            pltpu.VMEM((heads, span, HEAD_SIZE), jnp.bfloat16),
            pltpu.VMEM((heads, span, 1), jnp.float32),
            pltpu.VMEM((heads, span, 2 * HEAD_SIZE), jnp.float32),
            pltpu.VMEM((heads, span, CORES * span), jnp.float32),
        ],
        compiler_params=params(40),
        cost_estimate=cost(8 * span * keys * width, 4 * keys * HEAD_SIZE, span * keys * heads),
        name="attention",
    )(where, queries, query_gain, kv_own, kv_other, gates)


def project_kernel(where_ref, *refs):
    pieces, (weight_ref, out_ref) = refs[:-2], refs[-2:]
    n_tp = len(pieces)
    total = jnp.zeros(out_ref.shape, jnp.float32)
    for k in range(n_tp):
        source = (where_ref[0] + n_tp - k) & (n_tp - 1)
        total = total + jnp.dot(
            pieces[k][...], weight_ref[source], preferred_element_type=jnp.float32
        )
    out_ref[...] = total.astype(jnp.bfloat16)


def project(where, pieces, weight):
    rows, width = pieces[0].shape
    depth = weight.shape[2]
    return pl.pallas_call(
        project_kernel,
        out_shape=jax.ShapeDtypeStruct((rows, depth), jnp.bfloat16),
        in_specs=[SMEM] + [VMEM] * (len(pieces) + 1),
        out_specs=VMEM,
        compiler_params=params(24),
        cost_estimate=cost(
            2 * len(pieces) * rows * width * depth, 2 * len(pieces) * width * depth
        ),
        name="project",
    )(where, *pieces, weight)


def shard_moves(n_tp):
    at = lambda core, t: core * n_tp + t
    near, over, up = [], [], []
    for core in range(CORES):
        for t in range(n_tp):
            if t // 2 == core:
                near.append((at(core, t), at(0, t ^ 1)))
                over.append((at(core, t), at(1 - core, t)))
            else:
                near.append((at(core, t), at(1, n_tp - 1 - t)))
    swap = [(at(c, t), at(1 - c, t)) for c in range(CORES) for t in range(n_tp)]
    pair = [(at(1, t), at(1, t ^ 1)) for t in range(n_tp)]
    down = [(at(1, t), at(0, t)) for t in range(n_tp)]
    return near, over, swap, pair, down


def on_device(
    queries,
    key_rows,
    value_rows,
    query_gain,
    key_gain,
    log_forget,
    out_weight,
    expert_rows,
    expert_gain,
    routes,
    route_weight,
    gate_weight,
    up_weight,
    down_weight,
):
    n_tp = lax.axis_size("tp")
    chips = lax.axis_size("ep_0")
    chip, core, tp_index = (lax.axis_index(a) for a in ("ep_0", "ep_1", "tp"))
    where = jnp.stack([tp_index, core, chip]).astype(jnp.int32)
    span_rows, model_width = expert_rows.shape
    capacity = n_tp * ((3 * (span_rows // n_tp) * TOP + 2 * EXPERTS - 1) // (2 * EXPERTS))
    half = capacity // 2
    row = ("ep_1", "tp")

    near, over, swap, pair, down = shard_moves(n_tp)
    mine = (gate_weight[0], up_weight[0], down_weight[0])
    near_w = [lax.ppermute(w, row, near) for w in mine]
    over_w = [lax.ppermute(w, row, over) for w in mine]
    swap_w = [lax.ppermute(w, row, swap) for w in near_w]
    pair_w = [lax.ppermute(w, row, pair) for w in near_w]
    down_w = [lax.ppermute(w, row, down) for w in pair_w]
    shards = [*mine, *over_w, *near_w, *swap_w, *pair_w, *down_w]

    message = dispatch_rows(where, expert_rows, expert_gain.reshape(1, -1), routes, half)
    arrived = lax.all_to_all(
        message.reshape(chips, half, model_width), "ep_0", split_axis=0, concat_axis=0, tiled=True
    )
    outs = expert_rows_out(where, arrived.reshape(chips * half, model_width), shards, n_tp)

    def turn(parts):
        return [parts[0]] + [
            lax.ppermute(parts[k], "tp", [(t, (t + k) % n_tp) for t in range(n_tp)])
            for k in range(1, n_tp)
        ]

    def joined(parts):
        return jnp.stack([part.reshape(chips, half, part.shape[1]) for part in turn(parts)], axis=1)

    def send_back(table):
        return lax.all_to_all(table, "ep_0", split_axis=0, concat_axis=0, tiled=True)

    first = send_back(joined(outs[:n_tp]))
    second = joined(outs[n_tp:])

    k_normed = head_norm(key_rows, key_gain).astype(jnp.bfloat16)
    kv_own = lax.all_gather(
        jnp.concatenate([k_normed, value_rows], axis=1), "ep_0", axis=0, tiled=False
    )
    first, second, queries, kv_own = lax.optimization_barrier((first, second, queries, kv_own))
    second = send_back(second)
    kv_other = lax.ppermute(kv_own, "ep_1", [(0, 1), (1, 0)])
    attended = attention(
        where, queries, query_gain.reshape(1, -1), kv_own, kv_other, log_forget, n_tp
    )
    pieces = turn([attended[k] for k in range(n_tp)])
    mixer_out = project(where, pieces, lax.all_gather(out_weight, "tp", axis=0, tiled=False))
    second, mixer_out = lax.optimization_barrier((second, mixer_out))

    tables = [part.reshape(EXPERTS * capacity, part.shape[-1]) for part in (first, second)]
    expert_out = combine_rows(where, tables, routes.T, route_weight.T, half, n_tp)
    return (mixer_out, expert_out)


def solution(mesh):
    split = Mesh(
        mesh.devices.reshape(
            mesh.shape["grp"], mesh.shape["ep"] // CORES, CORES, mesh.shape["tp"]
        ),
        ("grp", "ep_0", "ep_1", "tp"),
    )
    in_specs = (
        P(GRP_EP, "tp"),
        P(GRP_EP, "tp"),
        P(GRP_EP, "tp"),
        P(),
        P(),
        P("tp", "grp"),
        P("tp", None),
        P(GRP_EP, None),
        P(),
        P(None, GRP_EP),
        P(None, GRP_EP),
        P(EP, None, "tp"),
        P(EP, None, "tp"),
        P(EP, "tp", None),
    )
    out_specs = (P(GRP_EP_TP, None), P(GRP_EP, "tp"))
    return jax.shard_map(
        on_device, mesh=split, in_specs=in_specs, out_specs=out_specs, check_vma=False
    )
```

```python
import functools

import jax
import jax.numpy as jnp
from jax import lax
from jax.experimental import pallas as pl
from jax.experimental.pallas import tpu as pltpu
from jax.sharding import Mesh
from jax.sharding import PartitionSpec as P

HEAD_SIZE = 128
EXPERTS = 32
TOP = 2
CORES = 2
EP = ("ep_0", "ep_1")
GRP_EP = ("grp", "ep_0", "ep_1")
GRP_EP_TP = ("grp", "ep_0", "ep_1", "tp")
LOG2E = 1.4426950408889634
MIB = 1024 * 1024


SMEM = pl.BlockSpec(memory_space=pltpu.SMEM)
VMEM = pl.BlockSpec(memory_space=pltpu.VMEM)
HBM = pl.BlockSpec(memory_space=pltpu.HBM)


def cost(flops, bytes_accessed, transcendentals=0):
    return pl.CostEstimate(
        flops=int(flops), bytes_accessed=int(bytes_accessed), transcendentals=int(transcendentals)
    )


def params(limit_mib):
    return pltpu.CompilerParams(vmem_limit_bytes=limit_mib * MIB)


def head_norm(inputs, scale_gain):
    widened = inputs.astype(jnp.float32)
    factor = lax.rsqrt(jnp.mean(widened * widened, axis=-1, keepdims=True) + 1e-06)
    return widened * factor * scale_gain


def dispatch_kernel(
    half,
    where_ref,
    rows_ref,
    gain_ref,
    routes_ref,
    key_ref,
    value_ref,
    key_gain_ref,
    out_ref,
    kv_ref,
    normed_ref,
):
    tp_index = where_ref[0]
    kv_ref[:, :HEAD_SIZE] = head_norm(key_ref[...], key_gain_ref[...]).astype(jnp.bfloat16)
    kv_ref[:, HEAD_SIZE:] = value_ref[...]
    n_rows, width = rows_ref.shape
    step = 64

    def norm_step(i, carry):
        part = pl.ds(pl.multiple_of(i * step, step), step)
        normed_ref[part, :] = head_norm(rows_ref[part, :], gain_ref[...]).astype(jnp.bfloat16)
        return carry

    lax.fori_loop(0, n_rows // step, norm_step, 0)
    ids = routes_ref[...]
    expert_iota = lax.broadcasted_iota(jnp.int32, (EXPERTS, n_rows), 0)
    before = jnp.where(
        lax.broadcasted_iota(jnp.int32, (n_rows, n_rows), 0)
        < lax.broadcasted_iota(jnp.int32, (n_rows, n_rows), 1),
        1.0,
        0.0,
    ).astype(jnp.bfloat16)
    base = jnp.zeros((EXPERTS, 1), jnp.float32)
    targets = []
    for j in range(TOP):
        picked = ids[j : j + 1, :]
        one_hot = jnp.where(expert_iota == picked, 1.0, 0.0)
        rank = base + jnp.dot(
            one_hot.astype(jnp.bfloat16), before, preferred_element_type=jnp.float32
        )
        within = jnp.sum(one_hot * rank, axis=0, keepdims=True).astype(jnp.int32)
        base = base + jnp.sum(one_hot, axis=1, keepdims=True)
        low = (tp_index & 1) * half
        mine = ((picked & 1) == (tp_index >> 1)) & (within >= low) & (within < low + half)
        targets.append(jnp.where(mine, (picked >> 1) * half + within - low, -1))
    out_rows = out_ref.shape[0]
    row_iota = lax.broadcasted_iota(jnp.int32, (out_rows, n_rows), 0)
    select = jnp.where((row_iota == targets[0]) | (row_iota == targets[1]), 1.0, 0.0).astype(
        jnp.bfloat16
    )
    span = 512
    for start in range(0, width, span):
        cols = slice(start, start + span)
        out_ref[:, cols] = jnp.dot(
            select, normed_ref[:, cols], preferred_element_type=jnp.float32
        ).astype(jnp.bfloat16)


def dispatch_rows(where, expert_rows, gain, routes, key_rows, value_rows, key_gain, half):
    n_rows, width = expert_rows.shape
    out_rows = EXPERTS // CORES * half
    return pl.pallas_call(
        functools.partial(dispatch_kernel, half),
        out_shape=(
            jax.ShapeDtypeStruct((out_rows, width), jnp.bfloat16),
            jax.ShapeDtypeStruct((n_rows, 2 * HEAD_SIZE), jnp.bfloat16),
        ),
        in_specs=[SMEM] + [VMEM] * 6,
        out_specs=(VMEM, VMEM),
        scratch_shapes=[pltpu.VMEM((n_rows, width), jnp.bfloat16)],
        compiler_params=params(60),
        cost_estimate=cost(2 * out_rows * n_rows * width, 2 * (n_rows + out_rows) * width),
        name="dispatch",
    )(where, expert_rows, gain, routes, key_rows, value_rows, key_gain)


def combine_kernel(half, n_tp, where_ref, table_ref, routes_ref, weight_ref, out_ref):
    tp_index = where_ref[0]
    n_rows = out_ref.shape[0]
    ids = routes_ref[...]
    expert_iota = lax.broadcasted_iota(jnp.int32, (n_rows, EXPERTS), 1)
    before = jnp.where(
        lax.broadcasted_iota(jnp.int32, (n_rows, n_rows), 1)
        < lax.broadcasted_iota(jnp.int32, (n_rows, n_rows), 0),
        1.0,
        0.0,
    ).astype(jnp.bfloat16)
    base = jnp.zeros((1, EXPERTS), jnp.float32)
    table_rows, width = table_ref.shape
    slot_iota = lax.broadcasted_iota(jnp.int32, (n_rows, table_rows), 1)
    selects = []
    for j in range(TOP):
        picked = ids[:, j : j + 1]
        one_hot = jnp.where(expert_iota == picked, 1.0, 0.0)
        rank = base + jnp.dot(
            before, one_hot.astype(jnp.bfloat16), preferred_element_type=jnp.float32
        )
        within = jnp.sum(one_hot * rank, axis=1, keepdims=True).astype(jnp.int32)
        base = base + jnp.sum(one_hot, axis=0, keepdims=True)
        upper = (within >= half).astype(jnp.int32)
        source = (picked & 1) * 2 + upper
        turn = (tp_index + n_tp - source) & (n_tp - 1)
        place = ((picked >> 1) * n_tp + turn) * half + within - upper * half
        selects.append(jnp.where(slot_iota == place, 1.0, 0.0).astype(jnp.bfloat16))
    total = jnp.zeros((n_rows, width), jnp.float32)
    for j in range(TOP):
        rows = jnp.dot(selects[j], table_ref[...], preferred_element_type=jnp.float32)
        total = total + weight_ref[:, j : j + 1] * rows
    out_ref[...] = total.astype(jnp.bfloat16)


def combine_rows(where, table, routes_t, weight_t, half, n_tp):
    n_rows = routes_t.shape[0]
    slots, width = table.shape
    return pl.pallas_call(
        functools.partial(combine_kernel, half, n_tp),
        out_shape=jax.ShapeDtypeStruct((n_rows, width), jnp.bfloat16),
        in_specs=[SMEM] + [VMEM] * 3,
        out_specs=VMEM,
        compiler_params=params(32),
        cost_estimate=cost(4 * n_rows * slots * width, 2 * slots * width),
        name="combine",
    )(where, table, routes_t, weight_t)


def expert_kernel(where_ref, x_ref, *refs):
    sources = [refs[3 * i : 3 * i + 3] for i in range(6)]
    outs = refs[18:-6]
    gate_buf, up_buf, down_buf, hidden_ref, acc_ref, sems = refs[-6:]
    bufs = (gate_buf, up_buf, down_buf)
    core, tp_index = where_ref[1], where_ref[0]
    home = core == (tp_index >> 1)

    def fetch(place, source):
        for i in range(3):
            pltpu.make_async_copy(source[i], bufs[i].at[place], sems.at[place, i]).start()

    pl.when(home)(lambda: fetch(0, sources[0]))
    pl.when(jnp.logical_not(home))(lambda: fetch(0, sources[1]))
    fetch(1, sources[2])
    fetch(2, sources[3])
    pl.when(core == 1)(lambda: fetch(3, sources[4]))
    pl.when(core == 0)(lambda: fetch(3, sources[5]))

    n_rows = x_ref.shape[0]
    depth = acc_ref.shape[1]
    half_rows = n_rows // 2
    acc_ref[...] = jnp.zeros_like(acc_ref)

    def shard(p, carry):
        for i in range(3):
            pltpu.make_async_copy(sources[2][i], bufs[i].at[p], sems.at[p, i]).wait()
        for part in range(2):
            rows = slice(part * half_rows, (part + 1) * half_rows)
            x = x_ref[rows, :]
            gate = jnp.dot(x, gate_buf[p], preferred_element_type=jnp.float32)
            up = jnp.dot(x, up_buf[p], preferred_element_type=jnp.float32)
            hidden_ref[rows, :] = (gate / (1.0 + jnp.exp(-gate)) * up).astype(jnp.bfloat16)
        for start in range(0, depth, 512):
            cols = slice(start, start + 512)
            piece = jnp.dot(
                hidden_ref[...], down_buf[p, :, cols], preferred_element_type=jnp.float32
            )
            acc_ref[:, cols] += piece.astype(jnp.bfloat16).astype(jnp.float32)
        return carry

    lax.fori_loop(0, gate_buf.shape[0], shard, 0)
    n_tp = gate_buf.shape[0]
    width = outs[0].shape[1]
    for k in range(n_tp):
        start = ((tp_index + k) & (n_tp - 1)) * width
        cols = pl.ds(pl.multiple_of(start, width), width)
        outs[k][...] = acc_ref[:, cols].astype(jnp.bfloat16)


def expert_rows_out(where, x, shards, n_tp):
    n_rows, depth = x.shape
    ff_part = shards[0].shape[1]
    width = depth // n_tp
    out = jax.ShapeDtypeStruct((n_rows, width), jnp.bfloat16)
    return pl.pallas_call(
        expert_kernel,
        out_shape=[out] * n_tp,
        in_specs=[SMEM, VMEM] + [HBM] * len(shards),
        out_specs=[VMEM] * n_tp,
        scratch_shapes=[
            pltpu.VMEM((n_tp, depth, ff_part), jnp.bfloat16),
            pltpu.VMEM((n_tp, depth, ff_part), jnp.bfloat16),
            pltpu.VMEM((n_tp, ff_part, depth), jnp.bfloat16),
            pltpu.VMEM((n_rows, ff_part), jnp.bfloat16),
            pltpu.VMEM((n_rows, depth), jnp.float32),
            pltpu.SemaphoreType.DMA((n_tp, 3)),
        ],
        compiler_params=params(60),
        cost_estimate=cost(
            6 * n_rows * depth * ff_part * n_tp, 6 * n_tp * depth * ff_part + 4 * n_rows * depth
        ),
        name="experts",
    )(where, x, *shards)


def attention_kernel(
    where_ref, q_ref, gain_ref, own_ref, other_ref, gates_ref, out_ref, q_buf, max_ref, acc_ref, logit_ref
):
    chip, core = where_ref[2], where_ref[1]
    span = q_ref.shape[0]
    heads = q_ref.shape[1] // HEAD_SIZE
    scale = HEAD_SIZE ** (-0.5) * LOG2E
    my_block = chip * CORES + core

    def gate_row(r, block):
        return gates_ref[r : r + 1, pl.ds(pl.multiple_of(block * span, span), span)]

    origin = []
    for r in range(heads):
        cols = slice(r * HEAD_SIZE, (r + 1) * HEAD_SIZE)
        q_buf[r] = head_norm(q_ref[:, cols], gain_ref[...]).astype(jnp.bfloat16)
        origin.append(gate_row(r, my_block)[:, 0:1])

    def scores(r, kv_ref, place, block):
        product = lax.dot_general(
            q_buf[r],
            kv_ref[place, :, 0:HEAD_SIZE],
            (((1,), (1,)), ((), ())),
            preferred_element_type=jnp.float32,
        )
        return product * scale + (origin[r] - gate_row(r, block)) * LOG2E

    def weighted(prob, kv_ref, place):
        values = kv_ref[place, :, HEAD_SIZE : 2 * HEAD_SIZE]
        return jnp.dot(
            prob.astype(jnp.bfloat16),
            jnp.concatenate([values, jnp.ones_like(values)], axis=1),
            preferred_element_type=jnp.float32,
        )

    def first(r):
        logits = scores(r, own_ref, chip, my_block)
        row = lax.broadcasted_iota(jnp.int32, (span, span), 0)
        col = lax.broadcasted_iota(jnp.int32, (span, span), 1)
        logits = jnp.where(col <= row, logits, -jnp.inf)
        top = jnp.max(logits, axis=1, keepdims=True)
        prob = jnp.exp2(logits - top)
        max_ref[r] = top
        acc_ref[r] = weighted(prob, own_ref, chip)

    def fill(r, place):
        for i, ref in enumerate((own_ref, other_ref)):
            block = place * CORES + (core if i == 0 else 1 - core)
            logit_ref[r, :, i * span : (i + 1) * span] = scores(r, ref, place, block)

    def absorb(r, logits, pieces):
        old = max_ref[r]
        top = jnp.maximum(old, jnp.max(logits, axis=1, keepdims=True))
        acc = jnp.exp2(old - top) * acc_ref[r]
        max_ref[r] = top
        prob = jnp.exp2(logits - top)
        for i, (ref, place) in enumerate(pieces):
            acc = acc + weighted(prob[:, i * span : (i + 1) * span], ref, place)
        acc_ref[r] = acc

    for r in range(heads):
        first(r)

    @pl.when(core == 1)
    def _():
        for r in range(heads):
            absorb(r, scores(r, other_ref, chip, my_block - 1), [(other_ref, chip)])

    fill(0, 0)

    def step(place, carry):
        pieces = [(own_ref, place), (other_ref, place)]
        for r in range(heads):
            if r + 1 < heads:
                fill(r + 1, place)
            absorb(r, logit_ref[r], pieces)
            if r + 1 == heads - 1:
                fill(0, jnp.minimum(place + 1, chip))
        return carry

    lax.fori_loop(0, chip, step, 0)
    n_tp, part = out_ref.shape[:2]
    for r in range(heads):
        cols = slice(r * HEAD_SIZE, (r + 1) * HEAD_SIZE)
        for k in range(n_tp):
            start = ((where_ref[0] + k) & (n_tp - 1)) * part
            rows = pl.ds(pl.multiple_of(start, part), part)
            out_ref[k, :, cols] = (
                acc_ref[r, rows, :HEAD_SIZE] / acc_ref[r, rows, HEAD_SIZE:]
            ).astype(jnp.bfloat16)


def attention(where, queries, query_gain, kv_own, kv_other, gates, n_tp):
    span, width = queries.shape
    heads = width // HEAD_SIZE
    keys = gates.shape[1]
    return pl.pallas_call(
        attention_kernel,
        out_shape=jax.ShapeDtypeStruct((n_tp, span // n_tp, width), jnp.bfloat16),
        in_specs=[SMEM] + [VMEM] * 5,
        out_specs=VMEM,
        scratch_shapes=[
            pltpu.VMEM((heads, span, HEAD_SIZE), jnp.bfloat16),
            pltpu.VMEM((heads, span, 1), jnp.float32),
            pltpu.VMEM((heads, span, 2 * HEAD_SIZE), jnp.float32),
            pltpu.VMEM((heads, span, CORES * span), jnp.float32),
        ],
        compiler_params=params(40),
        cost_estimate=cost(8 * span * keys * width, 4 * keys * HEAD_SIZE, span * keys * heads),
        name="attention",
    )(where, queries, query_gain, kv_own, kv_other, gates)


def project_kernel(where_ref, *refs):
    pieces, (weight_ref, out_ref) = refs[:-2], refs[-2:]
    n_tp = len(pieces)
    total = jnp.zeros(out_ref.shape, jnp.float32)
    for k in range(n_tp):
        source = (where_ref[0] + n_tp - k) & (n_tp - 1)
        total = total + jnp.dot(
            pieces[k][...], weight_ref[source], preferred_element_type=jnp.float32
        )
    out_ref[...] = total.astype(jnp.bfloat16)


def project(where, pieces, weight):
    rows, width = pieces[0].shape
    depth = weight.shape[2]
    return pl.pallas_call(
        project_kernel,
        out_shape=jax.ShapeDtypeStruct((rows, depth), jnp.bfloat16),
        in_specs=[SMEM] + [VMEM] * (len(pieces) + 1),
        out_specs=VMEM,
        compiler_params=params(24),
        cost_estimate=cost(
            2 * len(pieces) * rows * width * depth, 2 * len(pieces) * width * depth
        ),
        name="project",
    )(where, *pieces, weight)


def shard_moves(n_tp):
    at = lambda core, t: core * n_tp + t
    near, over, up = [], [], []
    for core in range(CORES):
        for t in range(n_tp):
            if t // 2 == core:
                near.append((at(core, t), at(0, t ^ 1)))
                over.append((at(core, t), at(1 - core, t)))
            else:
                near.append((at(core, t), at(1, n_tp - 1 - t)))
    swap = [(at(c, t), at(1 - c, t)) for c in range(CORES) for t in range(n_tp)]
    pair = [(at(1, t), at(1, t ^ 1)) for t in range(n_tp)]
    down = [(at(1, t), at(0, t)) for t in range(n_tp)]
    return near, over, swap, pair, down


def on_device(
    queries,
    key_rows,
    value_rows,
    query_gain,
    key_gain,
    log_forget,
    out_weight,
    expert_rows,
    expert_gain,
    routes,
    route_weight,
    gate_weight,
    up_weight,
    down_weight,
):
    n_tp = lax.axis_size("tp")
    chips = lax.axis_size("ep_0")
    chip, core, tp_index = (lax.axis_index(a) for a in ("ep_0", "ep_1", "tp"))
    where = jnp.stack([tp_index, core, chip]).astype(jnp.int32)
    span_rows, model_width = expert_rows.shape
    capacity = n_tp * ((3 * (span_rows // n_tp) * TOP + 2 * EXPERTS - 1) // (2 * EXPERTS))
    half = capacity // 2
    row = ("ep_1", "tp")

    near, over, swap, pair, down = shard_moves(n_tp)
    mine = (gate_weight[0], up_weight[0], down_weight[0])
    near_w = [lax.ppermute(w, row, near) for w in mine]
    over_w = [lax.ppermute(w, row, over) for w in mine]
    swap_w = [lax.ppermute(w, row, swap) for w in near_w]
    pair_w = [lax.ppermute(w, row, pair) for w in near_w]
    down_w = [lax.ppermute(w, row, down) for w in pair_w]
    shards = [*mine, *over_w, *near_w, *swap_w, *pair_w, *down_w]

    message, key_value = dispatch_rows(
        where,
        expert_rows,
        expert_gain.reshape(1, -1),
        routes,
        key_rows,
        value_rows,
        key_gain.reshape(1, -1),
        half,
    )
    arrived = lax.all_to_all(
        message.reshape(chips, half, model_width), "ep_0", split_axis=0, concat_axis=0, tiled=True
    )
    outs = expert_rows_out(where, arrived.reshape(chips * half, model_width), shards, n_tp)

    def turn(parts):
        return [parts[0]] + [
            lax.ppermute(parts[k], "tp", [(t, (t + k) % n_tp) for t in range(n_tp)])
            for k in range(1, n_tp)
        ]

    table = jnp.stack(
        [part.reshape(chips, half, part.shape[1]) for part in turn(outs)], axis=1
    )

    kv_own = lax.all_gather(key_value, "ep_0", axis=0, tiled=False)
    table, queries = lax.optimization_barrier((table, queries))
    back = lax.all_to_all(table, "ep_0", split_axis=0, concat_axis=0, tiled=True)
    kv_other = lax.ppermute(kv_own, "ep_1", [(0, 1), (1, 0)])
    attended = attention(
        where, queries, query_gain.reshape(1, -1), kv_own, kv_other, log_forget, n_tp
    )
    pieces = turn([attended[k] for k in range(n_tp)])
    mixer_out = project(where, pieces, lax.all_gather(out_weight, "tp", axis=0, tiled=False))
    back, mixer_out = lax.optimization_barrier((back, mixer_out))
    back = back.reshape(EXPERTS * capacity, back.shape[-1])
    expert_out = combine_rows(where, back, routes.T, route_weight.T, half, n_tp)
    return (mixer_out, expert_out)


def solution(mesh):
    split = Mesh(
        mesh.devices.reshape(
            mesh.shape["grp"], mesh.shape["ep"] // CORES, CORES, mesh.shape["tp"]
        ),
        ("grp", "ep_0", "ep_1", "tp"),
    )
    in_specs = (
        P(GRP_EP, "tp"),
        P(GRP_EP, "tp"),
        P(GRP_EP, "tp"),
        P(),
        P(),
        P("tp", "grp"),
        P("tp", None),
        P(GRP_EP, None),
        P(),
        P(None, GRP_EP),
        P(None, GRP_EP),
        P(EP, None, "tp"),
        P(EP, None, "tp"),
        P(EP, "tp", None),
    )
    out_specs = (P(GRP_EP_TP, None), P(GRP_EP, "tp"))
    return jax.shard_map(
        on_device, mesh=split, in_specs=in_specs, out_specs=out_specs, check_vma=False
    )
```

```python
import functools

import jax
import jax.numpy as jnp
from jax import lax
from jax.experimental import pallas as pl
from jax.experimental.pallas import tpu as pltpu
from jax.sharding import Mesh
from jax.sharding import PartitionSpec as P

HEAD_SIZE = 128
EXPERTS = 32
TOP = 2
CORES = 2
EP = ("ep_0", "ep_1")
GRP_EP = ("grp", "ep_0", "ep_1")
GRP_EP_TP = ("grp", "ep_0", "ep_1", "tp")
LOG2E = 1.4426950408889634
MIB = 1024 * 1024


SMEM = pl.BlockSpec(memory_space=pltpu.SMEM)
VMEM = pl.BlockSpec(memory_space=pltpu.VMEM)
HBM = pl.BlockSpec(memory_space=pltpu.HBM)


def cost(flops, bytes_accessed, transcendentals=0):
    return pl.CostEstimate(
        flops=int(flops), bytes_accessed=int(bytes_accessed), transcendentals=int(transcendentals)
    )


def params(limit_mib):
    return pltpu.CompilerParams(vmem_limit_bytes=limit_mib * MIB)


def head_norm(inputs, scale_gain):
    widened = inputs.astype(jnp.float32)
    factor = lax.rsqrt(jnp.mean(widened * widened, axis=-1, keepdims=True) + 1e-06)
    return widened * factor * scale_gain


def early_slots(half):
    return half * 2 // 3


def dispatch_kernel(
    half,
    where_ref,
    rows_ref,
    gain_ref,
    routes_ref,
    key_ref,
    value_ref,
    key_gain_ref,
    early_ref,
    late_ref,
    kv_ref,
    normed_ref,
):
    tp_index = where_ref[0]
    early = early_slots(half)
    early_rows = early_ref.shape[0]
    kv_ref[:, :HEAD_SIZE] = head_norm(key_ref[...], key_gain_ref[...]).astype(jnp.bfloat16)
    kv_ref[:, HEAD_SIZE:] = value_ref[...]
    n_rows, width = rows_ref.shape
    step = 64

    def norm_step(i, carry):
        part = pl.ds(pl.multiple_of(i * step, step), step)
        normed_ref[part, :] = head_norm(rows_ref[part, :], gain_ref[...]).astype(jnp.bfloat16)
        return carry

    lax.fori_loop(0, n_rows // step, norm_step, 0)
    ids = routes_ref[...]
    expert_iota = lax.broadcasted_iota(jnp.int32, (EXPERTS, n_rows), 0)
    before = jnp.where(
        lax.broadcasted_iota(jnp.int32, (n_rows, n_rows), 0)
        < lax.broadcasted_iota(jnp.int32, (n_rows, n_rows), 1),
        1.0,
        0.0,
    ).astype(jnp.bfloat16)
    base = jnp.zeros((EXPERTS, 1), jnp.float32)
    targets = []
    for j in range(TOP):
        picked = ids[j : j + 1, :]
        one_hot = jnp.where(expert_iota == picked, 1.0, 0.0)
        rank = base + jnp.dot(
            one_hot.astype(jnp.bfloat16), before, preferred_element_type=jnp.float32
        )
        within = jnp.sum(one_hot * rank, axis=0, keepdims=True).astype(jnp.int32)
        base = base + jnp.sum(one_hot, axis=1, keepdims=True)
        low = (tp_index & 1) * half
        mine = ((picked & 1) == (tp_index >> 1)) & (within >= low) & (within < low + half)
        slot = within - low
        place = jnp.where(
            slot < early,
            (picked >> 1) * early + slot,
            early_rows + (picked >> 1) * (half - early) + slot - early,
        )
        targets.append(jnp.where(mine, place, -1))
    out_rows = early_rows + late_ref.shape[0]
    row_iota = lax.broadcasted_iota(jnp.int32, (out_rows, n_rows), 0)
    select = jnp.where((row_iota == targets[0]) | (row_iota == targets[1]), 1.0, 0.0).astype(
        jnp.bfloat16
    )
    span = 512
    for start in range(0, width, span):
        cols = slice(start, start + span)
        rows = jnp.dot(select, normed_ref[:, cols], preferred_element_type=jnp.float32)
        rows = rows.astype(jnp.bfloat16)
        early_ref[:, cols] = rows[:early_rows]
        late_ref[:, cols] = rows[early_rows:]


def dispatch_rows(where, expert_rows, gain, routes, key_rows, value_rows, key_gain, half):
    n_rows, width = expert_rows.shape
    out_rows = EXPERTS // CORES * half
    early_rows = EXPERTS // CORES * early_slots(half)
    return pl.pallas_call(
        functools.partial(dispatch_kernel, half),
        out_shape=(
            jax.ShapeDtypeStruct((early_rows, width), jnp.bfloat16),
            jax.ShapeDtypeStruct((out_rows - early_rows, width), jnp.bfloat16),
            jax.ShapeDtypeStruct((n_rows, 2 * HEAD_SIZE), jnp.bfloat16),
        ),
        in_specs=[SMEM] + [VMEM] * 6,
        out_specs=(VMEM, VMEM, VMEM),
        scratch_shapes=[pltpu.VMEM((n_rows, width), jnp.bfloat16)],
        compiler_params=params(60),
        cost_estimate=cost(2 * out_rows * n_rows * width, 2 * (n_rows + out_rows) * width),
        name="dispatch",
    )(where, expert_rows, gain, routes, key_rows, value_rows, key_gain)


def combine_kernel(half, n_tp, where_ref, early_ref, late_ref, routes_ref, weight_ref, out_ref):
    early = early_slots(half)
    tp_index = where_ref[0]
    n_rows = out_ref.shape[0]
    ids = routes_ref[...]
    expert_iota = lax.broadcasted_iota(jnp.int32, (n_rows, EXPERTS), 1)
    before = jnp.where(
        lax.broadcasted_iota(jnp.int32, (n_rows, n_rows), 1)
        < lax.broadcasted_iota(jnp.int32, (n_rows, n_rows), 0),
        1.0,
        0.0,
    ).astype(jnp.bfloat16)
    base = jnp.zeros((1, EXPERTS), jnp.float32)
    width = early_ref.shape[1]
    total = jnp.zeros((n_rows, width), jnp.float32)
    for j in range(TOP):
        picked = ids[:, j : j + 1]
        one_hot = jnp.where(expert_iota == picked, 1.0, 0.0)
        rank = base + jnp.dot(
            before, one_hot.astype(jnp.bfloat16), preferred_element_type=jnp.float32
        )
        within = jnp.sum(one_hot * rank, axis=1, keepdims=True).astype(jnp.int32)
        base = base + jnp.sum(one_hot, axis=0, keepdims=True)
        upper = (within >= half).astype(jnp.int32)
        source = (picked & 1) * 2 + upper
        turn = (tp_index + n_tp - source) & (n_tp - 1)
        group = (picked >> 1) * n_tp + turn
        slot = within - upper * half
        rows = jnp.zeros((n_rows, width), jnp.float32)
        for table_ref, here, place in (
            (early_ref, slot < early, group * early + slot),
            (late_ref, slot >= early, group * (half - early) + slot - early),
        ):
            iota = lax.broadcasted_iota(jnp.int32, (n_rows, table_ref.shape[0]), 1)
            select = jnp.where(iota == jnp.where(here, place, -1), 1.0, 0.0).astype(jnp.bfloat16)
            rows = rows + jnp.dot(select, table_ref[...], preferred_element_type=jnp.float32)
        total = total + weight_ref[:, j : j + 1] * rows
    out_ref[...] = total.astype(jnp.bfloat16)


def combine_rows(where, tables, routes_t, weight_t, half, n_tp):
    n_rows = routes_t.shape[0]
    slots, width = sum(t.shape[0] for t in tables), tables[0].shape[1]
    return pl.pallas_call(
        functools.partial(combine_kernel, half, n_tp),
        out_shape=jax.ShapeDtypeStruct((n_rows, width), jnp.bfloat16),
        in_specs=[SMEM] + [VMEM] * 4,
        out_specs=VMEM,
        compiler_params=params(32),
        cost_estimate=cost(4 * n_rows * slots * width, 2 * slots * width),
        name="combine",
    )(where, *tables, routes_t, weight_t)


def expert_kernel(where_ref, x_ref, *refs):
    sources = [refs[3 * i : 3 * i + 3] for i in range(6)]
    outs = refs[18:-6]
    gate_buf, up_buf, down_buf, hidden_ref, acc_ref, sems = refs[-6:]
    bufs = (gate_buf, up_buf, down_buf)
    core, tp_index = where_ref[1], where_ref[0]
    home = core == (tp_index >> 1)

    def fetch(place, source):
        for i in range(3):
            pltpu.make_async_copy(source[i], bufs[i].at[place], sems.at[place, i]).start()

    pl.when(home)(lambda: fetch(0, sources[0]))
    pl.when(jnp.logical_not(home))(lambda: fetch(0, sources[1]))
    fetch(1, sources[2])
    fetch(2, sources[3])
    pl.when(core == 1)(lambda: fetch(3, sources[4]))
    pl.when(core == 0)(lambda: fetch(3, sources[5]))

    n_rows = x_ref.shape[0]
    depth = acc_ref.shape[1]
    half_rows = n_rows // 2
    acc_ref[...] = jnp.zeros_like(acc_ref)

    def shard(p, carry):
        for i in range(3):
            pltpu.make_async_copy(sources[2][i], bufs[i].at[p], sems.at[p, i]).wait()
        for part in range(2):
            rows = slice(part * half_rows, (part + 1) * half_rows)
            x = x_ref[rows, :]
            gate = jnp.dot(x, gate_buf[p], preferred_element_type=jnp.float32)
            up = jnp.dot(x, up_buf[p], preferred_element_type=jnp.float32)
            hidden_ref[rows, :] = (gate / (1.0 + jnp.exp(-gate)) * up).astype(jnp.bfloat16)
        for start in range(0, depth, 512):
            cols = slice(start, start + 512)
            piece = jnp.dot(
                hidden_ref[...], down_buf[p, :, cols], preferred_element_type=jnp.float32
            )
            acc_ref[:, cols] += piece.astype(jnp.bfloat16).astype(jnp.float32)
        return carry

    lax.fori_loop(0, gate_buf.shape[0], shard, 0)
    n_tp = gate_buf.shape[0]
    width = outs[0].shape[1]
    for k in range(n_tp):
        start = ((tp_index + k) & (n_tp - 1)) * width
        cols = pl.ds(pl.multiple_of(start, width), width)
        outs[k][...] = acc_ref[:, cols].astype(jnp.bfloat16)


def expert_rows_out(where, x, shards, n_tp):
    n_rows, depth = x.shape
    ff_part = shards[0].shape[1]
    width = depth // n_tp
    out = jax.ShapeDtypeStruct((n_rows, width), jnp.bfloat16)
    return pl.pallas_call(
        expert_kernel,
        out_shape=[out] * n_tp,
        in_specs=[SMEM, VMEM] + [HBM] * len(shards),
        out_specs=[VMEM] * n_tp,
        scratch_shapes=[
            pltpu.VMEM((n_tp, depth, ff_part), jnp.bfloat16),
            pltpu.VMEM((n_tp, depth, ff_part), jnp.bfloat16),
            pltpu.VMEM((n_tp, ff_part, depth), jnp.bfloat16),
            pltpu.VMEM((n_rows, ff_part), jnp.bfloat16),
            pltpu.VMEM((n_rows, depth), jnp.float32),
            pltpu.SemaphoreType.DMA((n_tp, 3)),
        ],
        compiler_params=params(60),
        cost_estimate=cost(
            6 * n_rows * depth * ff_part * n_tp, 6 * n_tp * depth * ff_part + 4 * n_rows * depth
        ),
        name="experts",
    )(where, x, *shards)


def attention_kernel(
    where_ref, q_ref, gain_ref, own_ref, other_ref, gates_ref, out_ref, q_buf, max_ref, acc_ref, logit_ref
):
    chip, core = where_ref[2], where_ref[1]
    span = q_ref.shape[0]
    heads = q_ref.shape[1] // HEAD_SIZE
    scale = HEAD_SIZE ** (-0.5) * LOG2E
    my_block = chip * CORES + core

    def gate_row(r, block):
        return gates_ref[r : r + 1, pl.ds(pl.multiple_of(block * span, span), span)]

    origin = []
    for r in range(heads):
        cols = slice(r * HEAD_SIZE, (r + 1) * HEAD_SIZE)
        q_buf[r] = head_norm(q_ref[:, cols], gain_ref[...]).astype(jnp.bfloat16)
        origin.append(gate_row(r, my_block)[:, 0:1])

    def scores(r, kv_ref, place, block):
        product = lax.dot_general(
            q_buf[r],
            kv_ref[place, :, 0:HEAD_SIZE],
            (((1,), (1,)), ((), ())),
            preferred_element_type=jnp.float32,
        )
        return product * scale + (origin[r] - gate_row(r, block)) * LOG2E

    def weighted(prob, kv_ref, place):
        values = kv_ref[place, :, HEAD_SIZE : 2 * HEAD_SIZE]
        return jnp.dot(
            prob.astype(jnp.bfloat16),
            jnp.concatenate([values, jnp.ones_like(values)], axis=1),
            preferred_element_type=jnp.float32,
        )

    def first(r):
        logits = scores(r, own_ref, chip, my_block)
        row = lax.broadcasted_iota(jnp.int32, (span, span), 0)
        col = lax.broadcasted_iota(jnp.int32, (span, span), 1)
        logits = jnp.where(col <= row, logits, -jnp.inf)
        top = jnp.max(logits, axis=1, keepdims=True)
        prob = jnp.exp2(logits - top)
        max_ref[r] = top
        acc_ref[r] = weighted(prob, own_ref, chip)

    def fill(r, place):
        for i, ref in enumerate((own_ref, other_ref)):
            block = place * CORES + (core if i == 0 else 1 - core)
            logit_ref[r, :, i * span : (i + 1) * span] = scores(r, ref, place, block)

    def absorb(r, logits, pieces):
        old = max_ref[r]
        top = jnp.maximum(old, jnp.max(logits, axis=1, keepdims=True))
        acc = jnp.exp2(old - top) * acc_ref[r]
        max_ref[r] = top
        prob = jnp.exp2(logits - top)
        for i, (ref, place) in enumerate(pieces):
            acc = acc + weighted(prob[:, i * span : (i + 1) * span], ref, place)
        acc_ref[r] = acc

    for r in range(heads):
        first(r)

    @pl.when(core == 1)
    def _():
        for r in range(heads):
            absorb(r, scores(r, other_ref, chip, my_block - 1), [(other_ref, chip)])

    fill(0, 0)

    def step(place, carry):
        pieces = [(own_ref, place), (other_ref, place)]
        for r in range(heads):
            if r + 1 < heads:
                fill(r + 1, place)
            absorb(r, logit_ref[r], pieces)
            if r + 1 == heads - 1:
                fill(0, jnp.minimum(place + 1, chip))
        return carry

    lax.fori_loop(0, chip, step, 0)
    n_tp, part = out_ref.shape[:2]
    for r in range(heads):
        cols = slice(r * HEAD_SIZE, (r + 1) * HEAD_SIZE)
        for k in range(n_tp):
            start = ((where_ref[0] + k) & (n_tp - 1)) * part
            rows = pl.ds(pl.multiple_of(start, part), part)
            out_ref[k, :, cols] = (
                acc_ref[r, rows, :HEAD_SIZE] / acc_ref[r, rows, HEAD_SIZE:]
            ).astype(jnp.bfloat16)


def attention(where, queries, query_gain, kv_own, kv_other, gates, n_tp):
    span, width = queries.shape
    heads = width // HEAD_SIZE
    keys = gates.shape[1]
    return pl.pallas_call(
        attention_kernel,
        out_shape=jax.ShapeDtypeStruct((n_tp, span // n_tp, width), jnp.bfloat16),
        in_specs=[SMEM] + [VMEM] * 5,
        out_specs=VMEM,
        scratch_shapes=[
            pltpu.VMEM((heads, span, HEAD_SIZE), jnp.bfloat16),
            pltpu.VMEM((heads, span, 1), jnp.float32),
            pltpu.VMEM((heads, span, 2 * HEAD_SIZE), jnp.float32),
            pltpu.VMEM((heads, span, CORES * span), jnp.float32),
        ],
        compiler_params=params(40),
        cost_estimate=cost(8 * span * keys * width, 4 * keys * HEAD_SIZE, span * keys * heads),
        name="attention",
    )(where, queries, query_gain, kv_own, kv_other, gates)


def project_kernel(where_ref, *refs):
    pieces, (weight_ref, out_ref) = refs[:-2], refs[-2:]
    n_tp = len(pieces)
    total = jnp.zeros(out_ref.shape, jnp.float32)
    for k in range(n_tp):
        source = (where_ref[0] + n_tp - k) & (n_tp - 1)
        total = total + jnp.dot(
            pieces[k][...], weight_ref[source], preferred_element_type=jnp.float32
        )
    out_ref[...] = total.astype(jnp.bfloat16)


def project(where, pieces, weight):
    rows, width = pieces[0].shape
    depth = weight.shape[2]
    return pl.pallas_call(
        project_kernel,
        out_shape=jax.ShapeDtypeStruct((rows, depth), jnp.bfloat16),
        in_specs=[SMEM] + [VMEM] * (len(pieces) + 1),
        out_specs=VMEM,
        compiler_params=params(24),
        cost_estimate=cost(
            2 * len(pieces) * rows * width * depth, 2 * len(pieces) * width * depth
        ),
        name="project",
    )(where, *pieces, weight)


def shard_moves(n_tp):
    at = lambda core, t: core * n_tp + t
    near, over, up = [], [], []
    for core in range(CORES):
        for t in range(n_tp):
            if t // 2 == core:
                near.append((at(core, t), at(0, t ^ 1)))
                over.append((at(core, t), at(1 - core, t)))
            else:
                near.append((at(core, t), at(1, n_tp - 1 - t)))
    swap = [(at(c, t), at(1 - c, t)) for c in range(CORES) for t in range(n_tp)]
    pair = [(at(1, t), at(1, t ^ 1)) for t in range(n_tp)]
    down = [(at(1, t), at(0, t)) for t in range(n_tp)]
    return near, over, swap, pair, down


def on_device(
    queries,
    key_rows,
    value_rows,
    query_gain,
    key_gain,
    log_forget,
    out_weight,
    expert_rows,
    expert_gain,
    routes,
    route_weight,
    gate_weight,
    up_weight,
    down_weight,
):
    n_tp = lax.axis_size("tp")
    chips = lax.axis_size("ep_0")
    chip, core, tp_index = (lax.axis_index(a) for a in ("ep_0", "ep_1", "tp"))
    where = jnp.stack([tp_index, core, chip]).astype(jnp.int32)
    span_rows, model_width = expert_rows.shape
    capacity = n_tp * ((3 * (span_rows // n_tp) * TOP + 2 * EXPERTS - 1) // (2 * EXPERTS))
    half = capacity // 2
    row = ("ep_1", "tp")

    near, over, swap, pair, down = shard_moves(n_tp)
    mine = (gate_weight[0], up_weight[0], down_weight[0])
    with jax.named_scope("near"):
        near_w = [lax.ppermute(w, row, near) for w in mine]
    over_w = [lax.ppermute(w, row, over) for w in mine]
    swap_w = [lax.ppermute(w, row, swap) for w in near_w]
    pair_w = [lax.ppermute(w, row, pair) for w in near_w]
    down_w = [lax.ppermute(w, row, down) for w in pair_w]
    shards = [*mine, *over_w, *near_w, *swap_w, *pair_w, *down_w]

    *messages, key_value = dispatch_rows(
        where,
        expert_rows,
        expert_gain.reshape(1, -1),
        routes,
        key_rows,
        value_rows,
        key_gain.reshape(1, -1),
        half,
    )
    def turn(parts):
        return [parts[0]] + [
            lax.ppermute(parts[k], "tp", [(t, (t + k) % n_tp) for t in range(n_tp)])
            for k in range(1, n_tp)
        ]

    def over_chips(parts):
        return lax.all_to_all(parts, "ep_0", split_axis=0, concat_axis=0, tiled=True)

    def table_of(arrived):
        outs = expert_rows_out(where, arrived.reshape(-1, model_width), shards, n_tp)
        parts = [part.reshape(chips, -1, part.shape[1]) for part in turn(outs)]
        return jnp.stack(parts, axis=1)

    messages = [m.reshape(chips, -1, model_width) for m in messages]
    with jax.named_scope("early_out"):
        early = over_chips(messages[0])
    late = over_chips(messages[1])
    early, late_message = table_of(early), late
    first = over_chips(early)
    late = table_of(late_message)

    kv_own = lax.all_gather(key_value, "ep_0", axis=0, tiled=False)
    first, late, queries, kv_own = lax.optimization_barrier((first, late, queries, kv_own))
    second = over_chips(late)
    kv_other = lax.ppermute(kv_own, "ep_1", [(0, 1), (1, 0)])
    attended = attention(
        where, queries, query_gain.reshape(1, -1), kv_own, kv_other, log_forget, n_tp
    )
    pieces = turn([attended[k] for k in range(n_tp)])
    mixer_out = project(where, pieces, lax.all_gather(out_weight, "tp", axis=0, tiled=False))
    second, mixer_out = lax.optimization_barrier((second, mixer_out))
    tables = [part.reshape(-1, part.shape[-1]) for part in (first, second)]
    expert_out = combine_rows(where, tables, routes.T, route_weight.T, half, n_tp)
    return (mixer_out, expert_out)


def solution(mesh):
    split = Mesh(
        mesh.devices.reshape(
            mesh.shape["grp"], mesh.shape["ep"] // CORES, CORES, mesh.shape["tp"]
        ),
        ("grp", "ep_0", "ep_1", "tp"),
    )
    in_specs = (
        P(GRP_EP, "tp"),
        P(GRP_EP, "tp"),
        P(GRP_EP, "tp"),
        P(),
        P(),
        P("tp", "grp"),
        P("tp", None),
        P(GRP_EP, None),
        P(),
        P(None, GRP_EP),
        P(None, GRP_EP),
        P(EP, None, "tp"),
        P(EP, None, "tp"),
        P(EP, "tp", None),
    )
    out_specs = (P(GRP_EP_TP, None), P(GRP_EP, "tp"))
    return jax.shard_map(
        on_device, mesh=split, in_specs=in_specs, out_specs=out_specs, check_vma=False
    )
```
